512 devices in a mesh: sp: 64 (over z, y), tp: 8 (over x, core).
Axes of the slice: x: 4, y: 4, z: 16, core: 2. Of those that a mesh axis runs over, the one named last changes fastest.
Arguments:
- queries: bfloat16 [8192, 1024], P('sp', 'tp'), may hold values from -6 to 6
- attn_out: bfloat16 [8192, 1024], P('sp', 'tp'), may hold values from -6 to 6
- out_grad: bfloat16 [8192, 1024], P('sp', 'tp'), may hold values from -384 to 384
- row_lse: float32 [8192, 8], P('sp', 'tp'), may hold values from 9.5 to 12.5
- source: bfloat16 [32768, 4096], P('sp', 'tp'), may hold values from -6 to 6
- saved_keys: bfloat16 [32768, 256], P('sp'), may hold values from -6 to 6
- saved_values: bfloat16 [32768, 256], P('sp'), may hold values from -6 to 6
- key_weight: bfloat16 [4096, 256], P('tp'), may hold values from -0.09375 to 0.09375
- value_weight: bfloat16 [4096, 256], P('tp'), may hold values from -0.09375 to 0.09375
Outputs:
- query_grad: float32 [8192, 1024], P('sp', 'tp')
- source_grad: float32 [32768, 4096], P('sp', 'tp')
- key_grad: float32 [256, 4096], P('sp', 'tp')
The draws below stay inside these ranges and needn't reach their ends.
All inputs are finite; a program needn't handle non-finite values.
Results may differ from the reference program's by a relative error of at most 0.012.
Values may be sent and summed in bfloat16 or wider, within the bound.
No kernel may reach another device: no remote copies, remote signals or barrier semaphores. Data moves between devices by JAX's collectives and lax.ppermute only.
A program may use at most 64 MiB of HBM per device.

```python
import math
import jax
import jax.numpy as jnp
from jax import lax

D = 4096
HEADS = 8
KV_HEADS = 2
HEAD_DIM = 128
TARGET_ROWS = 8192
SOURCE_ROWS = 32768


def levels(rng, extent, cuts, smallest, largest):
    def one(position, parts):
        heights = jax.random.uniform(jax.random.fold_in(jax.random.fold_in(rng, 6), position), (parts,), jnp.float32, smallest / len(cuts), largest / len(cuts))
        return jnp.repeat(jnp.exp(heights), extent[position] // parts).reshape((-1,) + (1,) * (len(extent) - position - 1))

    gain = one(*cuts[0])
    for cut in cuts[1:]:
        gain = gain * one(*cut)
    return gain


def normal_values(rng, dims, deviation, reach, pieces=(), dtype=jnp.bfloat16):
    array = deviation * jax.random.normal(rng, dims, jnp.float32)
    if pieces:
        array = array * levels(rng, dims, pieces, -0.22, 0.18)
    return jnp.clip(array, -reach, reach).astype(dtype)


def setup_inputs(seed: int = 0) -> dict:
    arg_keys = jax.random.split(jax.random.key(seed), 10)
    return {
        "queries": normal_values(arg_keys[0], (TARGET_ROWS, HEADS * HEAD_DIM), 1.0, 6.0, ((0, 64), (1, 8))),
        "attn_out": normal_values(arg_keys[1], (TARGET_ROWS, HEADS * HEAD_DIM), 1.0, 6.0, ((0, 64), (1, 8))),
        "out_grad": normal_values(arg_keys[2], (TARGET_ROWS, HEADS * HEAD_DIM), 64.0, 384.0, ((0, 64), (1, 8))),
        "row_lse": jnp.clip(9.5 + 3.0 * jax.random.uniform(arg_keys[3], (TARGET_ROWS, HEADS), jnp.float32) ** levels(arg_keys[3], (TARGET_ROWS, HEADS), ((0, 64), (1, 8)), -0.2, 0.2), 9.5, 12.5),
        "source": normal_values(arg_keys[4], (SOURCE_ROWS, D), 1.0, 6.0, ((0, 64), (1, 8))),
        "saved_keys": normal_values(arg_keys[5], (SOURCE_ROWS, KV_HEADS * HEAD_DIM), 1.0, 6.0, ((0, 64),)),
        "saved_values": normal_values(arg_keys[6], (SOURCE_ROWS, KV_HEADS * HEAD_DIM), 1.0, 6.0, ((0, 64),)),
        "key_weight": normal_values(arg_keys[7], (D, KV_HEADS * HEAD_DIM), D ** -0.5, 0.09375, ((0, 8),)),
        "value_weight": normal_values(arg_keys[8], (D, KV_HEADS * HEAD_DIM), D ** -0.5, 0.09375, ((0, 8),)),
    }


def reference(queries, attn_out, out_grad, row_lse, source, saved_keys, saved_values, key_weight, value_weight):
    per_key = HEADS // KV_HEADS
    score_scale = 1.0 / math.sqrt(HEAD_DIM)
    tgt_len = queries.shape[0]
    src_len = source.shape[0]
    span = math.gcd(tgt_len, 1024)
    count = tgt_len // span
    row_delta = lax.optimization_barrier(jnp.sum((out_grad.astype(jnp.float32) * attn_out.astype(jnp.float32)).reshape(-1, HEADS, HEAD_DIM), axis=2))
    key_acc = jnp.zeros((src_len, KV_HEADS * HEAD_DIM), jnp.float32)
    value_acc = jnp.zeros((src_len, KV_HEADS * HEAD_DIM), jnp.float32)
    head_parts = []
    for head_index in range(HEADS):
        kv_lo = head_index // per_key * HEAD_DIM
        col_lo = head_index * HEAD_DIM
        key_head = saved_keys[:, kv_lo:kv_lo + HEAD_DIM]
        value_head = saved_values[:, kv_lo:kv_lo + HEAD_DIM]
        query_blocks = queries[:, col_lo:col_lo + HEAD_DIM].reshape(count, span, HEAD_DIM)
        grad_blocks = out_grad[:, col_lo:col_lo + HEAD_DIM].reshape(count, span, HEAD_DIM)
        lse_blocks = row_lse[:, head_index:head_index + 1].reshape(count, span, 1)
        delta_blocks = row_delta[:, head_index:head_index + 1].reshape(count, span, 1)

        def step(carry, items):
            key_part, value_part = carry
            query_head, grad_head, lse_col, delta_col = items
            scores = jnp.dot(query_head, key_head.T, preferred_element_type=jnp.float32) * score_scale
            attn_probs = jnp.exp(scores - lse_col)
            dprobs = jnp.dot(grad_head, value_head.T, preferred_element_type=jnp.float32)
            dscores = (attn_probs * (dprobs - delta_col) * score_scale).astype(jnp.bfloat16)
            key_part = key_part + jnp.dot(dscores.T, query_head, preferred_element_type=jnp.float32)
            value_part = value_part + jnp.dot(attn_probs.astype(jnp.bfloat16).T, grad_head, preferred_element_type=jnp.float32)
            return ((key_part, value_part), jnp.dot(dscores, key_head, preferred_element_type=jnp.float32))
        empty = jnp.zeros((src_len, HEAD_DIM), jnp.float32)
        (key_part, value_part), query_blocks_out = lax.scan(step, (empty, empty), (query_blocks, grad_blocks, lse_blocks, delta_blocks))
        head_parts.append(query_blocks_out.reshape(tgt_len, HEAD_DIM))
        key_acc = key_acc.at[:, kv_lo:kv_lo + HEAD_DIM].add(key_part)
        value_acc = value_acc.at[:, kv_lo:kv_lo + HEAD_DIM].add(value_part)
    query_grad = jnp.concatenate(head_parts, axis=1)
    key_half = key_acc.astype(jnp.bfloat16)
    value_half = value_acc.astype(jnp.bfloat16)
    source_grad = jnp.dot(key_half, key_weight.T, preferred_element_type=jnp.float32) + jnp.dot(value_half, value_weight.T, preferred_element_type=jnp.float32)
    key_grad = jnp.dot(key_half.T, source, preferred_element_type=jnp.float32) * (1.0 / math.sqrt(source.shape[0]))
    return (query_grad, source_grad, key_grad)
```

```python
import math

import jax
import jax.numpy as jnp
from jax import lax
from jax.experimental import pallas as pl
from jax.experimental.pallas import tpu as pltpu
from jax.sharding import Mesh
from jax.sharding import PartitionSpec as P

HEAD_DIM = 128
SP = ("z", "y")
TP = ("g", "h", "c")
TEAM = ("y", "h", "c")
SPLIT = (16, 4, 2, 2, 2)
F32 = jnp.float32
BF16 = jnp.bfloat16
HEAD_ROWS = 112
STAT_ROWS = 16
VMEM_LIMIT = 56 * 2**20


def in_vmem():
    return pl.BlockSpec(memory_space=pltpu.VMEM)


def pieces(value):
    high = value.astype(BF16)
    rest = value - high.astype(F32)
    middle = rest.astype(BF16)
    low = (rest - middle.astype(F32)).astype(BF16)
    return [high, middle, low]


def pack_rows(queries, attn_out, out_grad, row_lse, saved_keys, saved_values):
    rows, width = queries.shape
    src = saved_keys.shape[0]
    z_count, y_count = (SPLIT[0], SPLIT[1])
    tail = rows - HEAD_ROWS

    def kernel(head_ref, q_ref, o_ref, do_ref, lse_ref, k_ref, v_ref, main_ref, small_ref, kv_ref):
        second = head_ref[0] > 0
        main_ref[:rows, :] = q_ref[...]
        main_ref[rows:, :] = do_ref[:HEAD_ROWS, :]
        product = do_ref[...].astype(F32) * o_ref[...].astype(F32)
        delta = jnp.sum(product.T, axis=0, keepdims=True)
        eye = lax.broadcasted_iota(jnp.int32, (rows, rows), 0) == lax.broadcasted_iota(
            jnp.int32, (rows, rows), 1
        )
        lse = jnp.sum(jnp.where(eye, lse_ref[...], 0.0), axis=0, keepdims=True)
        stats = pieces(lse * math.sqrt(HEAD_DIM)) + pieces(delta)
        line = lax.broadcasted_iota(jnp.int32, (STAT_ROWS, rows), 0)
        block = jnp.zeros((STAT_ROWS, rows), F32)
        for i, s in enumerate(stats):
            block = jnp.where(line == i, s.astype(F32), block)
        block = block.astype(BF16)
        last = do_ref[HEAD_ROWS:, :]
        for z in range(z_count):
            small_ref[z, :tail, :] = last
            small_ref[z, tail:, :] = block
        k = jnp.where(second, k_ref[:, HEAD_DIM:], k_ref[:, :HEAD_DIM])
        v = jnp.where(second, v_ref[:, HEAD_DIM:], v_ref[:, :HEAD_DIM])
        for y in range(y_count):
            kv_ref[y, :src, :] = k
            kv_ref[y, src:, :] = v

    return pl.pallas_call(
        kernel,
        in_specs=[pl.BlockSpec(memory_space=pltpu.SMEM)] + [in_vmem()] * 6,
        out_specs=[in_vmem()] * 3,
        out_shape=[
            jax.ShapeDtypeStruct((rows + HEAD_ROWS, width), BF16),
            jax.ShapeDtypeStruct((z_count, tail + STAT_ROWS, width), BF16),
            jax.ShapeDtypeStruct((y_count, 2 * src, HEAD_DIM), BF16),
        ],
        name="pack_rows",
    )(
        lax.axis_index("g").reshape(1),
        queries,
        attn_out,
        out_grad,
        row_lse,
        saved_keys,
        saved_values,
    )


def dot(left, right):
    return jnp.dot(left, right, preferred_element_type=F32)


def attention_backward(main, small, keyvals):
    z_count, main_rows, dim = main.shape
    y_count, src = (keyvals.shape[0], keyvals.shape[1] // 2)
    tail = small.shape[1] - STAT_ROWS
    rows = main_rows - (HEAD_DIM - tail)
    sources = y_count * src
    targets = z_count * rows
    scale = 1.0 / math.sqrt(HEAD_DIM)
    exp_scale = math.log2(math.e) * scale
    src_tile, tgt_tile, unroll = (512, 512, 4)
    src_tiles, tgt_tiles = (sources // src_tile, targets // tgt_tile)

    def kernel(
        main_ref, small_ref, kv_ref, dq_ref, dk_ref, dv_ref,
        k_wide, v_wide, k_turned, q_turned, do_turned, q_rows, do_rows, dk_acc, dv_acc, dq_acc,
    ):
        lane = lax.broadcasted_iota(jnp.int32, (src, dim), 1)
        lse_lanes = jnp.where(lane < 3, -1.0, 0.0).astype(BF16)
        delta_lanes = jnp.where((lane >= 3) & (lane < 6), -1.0, 0.0).astype(BF16)
        for y in range(y_count):
            at = slice(y * src, (y + 1) * src)
            k = kv_ref[y, :src, :]
            k_wide[at, :dim] = k
            k_wide[at, dim:] = lse_lanes
            v_wide[at, :dim] = kv_ref[y, src:, :]
            v_wide[at, dim:] = delta_lanes
            k_turned[:, at] = k.T
        for z in range(z_count):
            at = slice(z * rows, (z + 1) * rows)
            q = main_ref[z, :rows, :]
            do = jnp.concatenate([main_ref[z, rows:, :], small_ref[z, :tail, :]], axis=0)
            stats = small_ref[z, tail:, :]
            q_rows[at, :] = q
            do_rows[at, :] = do
            q_turned[:dim, at] = q.T
            do_turned[:dim, at] = do.T
            q_turned[dim : dim + STAT_ROWS, at] = stats
            do_turned[dim : dim + STAT_ROWS, at] = stats
        blank = jnp.zeros((dim - STAT_ROWS, targets), BF16)
        q_turned[dim + STAT_ROWS :, :] = blank
        do_turned[dim + STAT_ROWS :, :] = blank
        dk_acc[...] = jnp.zeros_like(dk_acc)
        dv_acc[...] = jnp.zeros_like(dv_acc)
        dq_acc[...] = jnp.zeros_like(dq_acc)

        def tile(s0, t0):
            s, t = (pl.ds(s0, src_tile), pl.ds(t0, tgt_tile))
            scores = dot(k_wide[s, :], q_turned[:, t])
            dprobs = dot(v_wide[s, :], do_turned[:, t])
            probs = jnp.exp2(scores * exp_scale)
            dscores = (probs * dprobs).astype(BF16)
            dv_acc[s, :] += dot(probs.astype(BF16), do_rows[t, :])
            dk_acc[s, :] += dot(dscores, q_rows[t, :])
            dq_acc[:, t] += dot(k_turned[:, s], dscores)

        def step(i, carry):
            s, t = (i // (tgt_tiles // unroll), i % (tgt_tiles // unroll))
            for u in range(unroll):
                tile(
                    pl.multiple_of(s * src_tile, src_tile),
                    pl.multiple_of((t * unroll + u) * tgt_tile, tgt_tile),
                )
            return carry

        lax.fori_loop(0, src_tiles * tgt_tiles // unroll, step, 0)
        dk_ref[...] = (dk_acc[...] * scale).astype(BF16)
        dv_ref[...] = dv_acc[...].astype(BF16)
        for z in range(z_count):
            dq_ref[z] = (dq_acc[:, z * rows : (z + 1) * rows] * scale).T.astype(BF16)

    return pl.pallas_call(
        kernel,
        in_specs=[in_vmem()] * 3,
        out_specs=[in_vmem()] * 3,
        out_shape=[
            jax.ShapeDtypeStruct((z_count, rows, dim), BF16),
            jax.ShapeDtypeStruct((sources, dim), BF16),
            jax.ShapeDtypeStruct((sources, dim), BF16),
        ],
        scratch_shapes=[
            pltpu.VMEM((sources, 2 * dim), BF16),
            pltpu.VMEM((sources, 2 * dim), BF16),
            pltpu.VMEM((dim, sources), BF16),
            pltpu.VMEM((2 * dim, targets), BF16),
            pltpu.VMEM((2 * dim, targets), BF16),
            pltpu.VMEM((targets, dim), BF16),
            pltpu.VMEM((targets, dim), BF16),
            pltpu.VMEM((sources, dim), F32),
            pltpu.VMEM((sources, dim), F32),
            pltpu.VMEM((dim, targets), F32),
        ],
        compiler_params=pltpu.CompilerParams(vmem_limit_bytes=VMEM_LIMIT),
        name="attention_backward",
    )(main, small, keyvals)


def added_up(arrived, copies):
    total = jnp.sum(arrived.astype(F32), axis=0).astype(BF16)
    return jnp.broadcast_to(total[None], (copies, *total.shape))


def exchanged(value, axes):
    return lax.all_to_all(value, axes, 0, 0, tiled=True)


def shards(
    queries, attn_out, out_grad, row_lse, source, saved_keys, saved_values, key_weight, value_weight
):
    src = source.shape[0]
    team = SPLIT[1] * SPLIT[3] * SPLIT[4]
    tp_count = SPLIT[2] * SPLIT[3] * SPLIT[4]
    sp_count = SPLIT[0] * SPLIT[1]
    weight_scale = 1.0 / math.sqrt(src * sp_count)
    main, small, keyvals = pack_rows(
        queries, attn_out, out_grad, row_lse, saved_keys, saved_values
    )
    keyvals = exchanged(keyvals, "y")
    small = exchanged(small, "z")
    main = lax.all_gather(main, "z", axis=0, tiled=False)
    dq, dk, dv = attention_backward(main, small, keyvals)

    dk_pieces = exchanged(dk.reshape(team, -1, HEAD_DIM), TEAM)
    key_half = exchanged(added_up(dk_pieces, tp_count), TP)
    dq_pieces = exchanged(dq, "z")
    dv_pieces = exchanged(dv.reshape(team, -1, HEAD_DIM), TEAM)
    value_half = exchanged(added_up(dv_pieces, tp_count), TP)

    key_half = key_half.reshape(2, src, HEAD_DIM)
    value_half = value_half.reshape(2, src, HEAD_DIM)
    key_terms = lax.dot_general(
        key_half, source, (((1,), (0,)), ((), ())), preferred_element_type=F32
    )
    key_terms = (key_terms * weight_scale).astype(BF16).reshape(sp_count, -1, source.shape[1])
    key_grad = jnp.sum(exchanged(key_terms, SP).astype(F32), axis=0)
    halves = [key_half[0], key_half[1], value_half[0], value_half[1]]
    weights = jnp.concatenate([key_weight, value_weight], axis=1)
    source_grad = lax.dot_general(
        jnp.concatenate(halves, axis=1),
        weights,
        (((1,), (1,)), ((), ())),
        preferred_element_type=F32,
    )
    query_grad = jnp.sum(dq_pieces.astype(F32), axis=0)
    return (query_grad, source_grad, key_grad)


def solution(mesh):
    split = Mesh(mesh.devices.reshape(SPLIT), ("z", "y", "g", "h", "c"))
    return jax.shard_map(
        shards,
        mesh=split,
        in_specs=(
            P(SP, TP),
            P(SP, TP),
            P(SP, TP),
            P(SP, TP),
            P(SP, TP),
            P(SP, None),
            P(SP, None),
            P(TP, None),
            P(TP, None),
        ),
        out_specs=(P(SP, TP), P(SP, TP), P(SP, TP)),
        check_vma=False,
    )
```

```python
import math

import jax
import jax.numpy as jnp
from jax import lax
from jax.experimental import pallas as pl
from jax.experimental.pallas import tpu as pltpu
from jax.sharding import Mesh
from jax.sharding import PartitionSpec as P


HEAD_DIM = 128
SP = ("z", "y")
TP = ("g", "h", "c")
TEAM = ("y", "h", "c")
SPLIT = (16, 4, 2, 2, 2)
F32 = jnp.float32
BF16 = jnp.bfloat16
HEAD_ROWS = 112
STAT_ROWS = 16
VMEM_LIMIT = 56 * 2**20


def in_vmem():
    return pl.BlockSpec(memory_space=pltpu.VMEM)


def pieces(value):
    high = value.astype(BF16)
    rest = value - high.astype(F32)
    middle = rest.astype(BF16)
    low = (rest - middle.astype(F32)).astype(BF16)
    return [high, middle, low]


def pack_rows(queries, attn_out, out_grad, row_lse, saved_keys, saved_values):
    rows, width = queries.shape
    src = saved_keys.shape[0]
    z_count = SPLIT[0]
    tail = rows - HEAD_ROWS

    def kernel(head_ref, q_ref, o_ref, do_ref, lse_ref, k_ref, v_ref, main_ref, small_ref, kv_ref):
        second = head_ref[0] > 0
        main_ref[:rows, :] = q_ref[...]
        main_ref[rows:, :] = do_ref[:HEAD_ROWS, :]
        product = do_ref[...].astype(F32) * o_ref[...].astype(F32)
        delta = jnp.sum(product.T, axis=0, keepdims=True)
        stats = pieces(lse_ref[...] * math.sqrt(HEAD_DIM)) + pieces(delta)
        line = lax.broadcasted_iota(jnp.int32, (STAT_ROWS, rows), 0)
        block = jnp.zeros((STAT_ROWS, rows), F32)
        for i, s in enumerate(stats):
            block = jnp.where(line == i, s.astype(F32), block)
        block = block.astype(BF16)
        last = do_ref[HEAD_ROWS:, :]
        for z in range(z_count):
            small_ref[z, :tail, :] = last
            small_ref[z, tail:, :] = block
        kv_ref[:src, :] = jnp.where(second, k_ref[:, HEAD_DIM:], k_ref[:, :HEAD_DIM])
        kv_ref[src:, :] = jnp.where(second, v_ref[:, HEAD_DIM:], v_ref[:, :HEAD_DIM])

    return pl.pallas_call(
        kernel,
        in_specs=[pl.BlockSpec(memory_space=pltpu.SMEM)] + [in_vmem()] * 6,
        out_specs=[in_vmem()] * 3,
        out_shape=[
            jax.ShapeDtypeStruct((rows + HEAD_ROWS, width), BF16),
            jax.ShapeDtypeStruct((z_count, tail + STAT_ROWS, width), BF16),
            jax.ShapeDtypeStruct((2 * src, HEAD_DIM), BF16),
        ],
        name="pack_rows",
    )(
        lax.axis_index("g").reshape(1),
        queries,
        attn_out,
        out_grad,
        row_lse.reshape(1, rows),
        saved_keys,
        saved_values,
    )


def dot(left, right):
    return jnp.dot(left, right, preferred_element_type=F32)


def attention_backward(place, main, small, keyvals):
    z_count, main_rows, dim = main.shape
    y_count, src = (len(keyvals), keyvals[0].shape[0] // 2)
    tail = small.shape[1] - STAT_ROWS
    rows = main_rows - (HEAD_DIM - tail)
    sources = y_count * src
    targets = z_count * rows
    scale = 1.0 / math.sqrt(HEAD_DIM)
    exp_scale = math.log2(math.e) * scale
    src_tile, tgt_tile, unroll = (512, 512, 4)
    src_tiles, tgt_tiles = (sources // src_tile, targets // tgt_tile)
    per_y = SPLIT[3] * SPLIT[4]
    team = y_count * per_y
    bits = z_count.bit_length() - 1

    def kernel(
        place_ref, main_ref, small_ref, kv0_ref, kv1_ref, kv2_ref, kv3_ref, send_ref, keep_ref, dkv_ref,
        k_wide, v_wide, k_turned, q_turned, do_turned, q_rows, do_rows, dk_acc, dv_acc, dq_acc,
    ):
        lane = lax.broadcasted_iota(jnp.int32, (src, dim), 1)
        lse_lanes = jnp.where(lane < 3, -1.0, 0.0).astype(BF16)
        delta_lanes = jnp.where((lane >= 3) & (lane < 6), -1.0, 0.0).astype(BF16)
        for y, kv_ref in enumerate((kv0_ref, kv1_ref, kv2_ref, kv3_ref)):
            at = slice(y * src, (y + 1) * src)
            k = kv_ref[:src, :]
            k_wide[at, :dim] = k
            k_wide[at, dim:] = lse_lanes
            v_wide[at, :dim] = kv_ref[src:, :]
            v_wide[at, dim:] = delta_lanes
            k_turned[:, at] = k.T
        for z in range(z_count):
            at = slice(z * rows, (z + 1) * rows)
            q = main_ref[z, :rows, :]
            do = jnp.concatenate([main_ref[z, rows:, :], small_ref[z, :tail, :]], axis=0)
            stats = small_ref[z, tail:, :]
            q_rows[at, :] = q
            do_rows[at, :] = do
            q_turned[:dim, at] = q.T
            do_turned[:dim, at] = do.T
            q_turned[dim : dim + STAT_ROWS, at] = stats
            do_turned[dim : dim + STAT_ROWS, at] = stats
        blank = jnp.zeros((dim - STAT_ROWS, targets), BF16)
        q_turned[dim + STAT_ROWS :, :] = blank
        do_turned[dim + STAT_ROWS :, :] = blank
        dk_acc[...] = jnp.zeros_like(dk_acc)
        dv_acc[...] = jnp.zeros_like(dv_acc)
        dq_acc[...] = jnp.zeros_like(dq_acc)

        def tile(s0, t0):
            s, t = (pl.ds(s0, src_tile), pl.ds(t0, tgt_tile))
            scores = dot(k_wide[s, :], q_turned[:, t])
            dprobs = dot(v_wide[s, :], do_turned[:, t])
            probs = jnp.exp2(scores * exp_scale)
            dscores = (probs * dprobs).astype(BF16)
            dv_acc[s, :] += dot(probs.astype(BF16), do_rows[t, :])
            dk_acc[s, :] += dot(dscores, q_rows[t, :])
            dq_acc[:, t] += dot(k_turned[:, s], dscores)

        def step(i, carry):
            s, t = (i // (tgt_tiles // unroll), i % (tgt_tiles // unroll))
            for u in range(unroll):
                tile(
                    pl.multiple_of(s * src_tile, src_tile),
                    pl.multiple_of((t * unroll + u) * tgt_tile, tgt_tile),
                )
            return carry

        lax.fori_loop(0, src_tiles * tgt_tiles // unroll, step, 0)
        me, y_me = (place_ref[0], place_ref[1])
        piece = sources // team
        for i in range(team):
            at = pl.multiple_of(((i // per_y + y_count - y_me) % y_count * per_y + i % per_y) * piece, piece)
            dkv_ref[i, :piece, :] = (dk_acc[pl.ds(at, piece), :] * scale).astype(BF16)
            dkv_ref[i, piece:, :] = dv_acc[pl.ds(at, piece), :].astype(BF16)
        for p in range(z_count):
            turned = sum(((p >> b) & 1) << (bits - 1 - b) for b in range(bits))
            at = pl.multiple_of(jnp.bitwise_xor(me, turned) * rows, rows)
            out = (dq_acc[:, pl.ds(at, rows)] * scale).T.astype(BF16)
            if p < z_count // 2:
                keep_ref[p] = out
            else:
                send_ref[p - z_count // 2] = out

    half = jax.ShapeDtypeStruct((z_count // 2, rows, dim), BF16)
    return pl.pallas_call(
        kernel,
        in_specs=[pl.BlockSpec(memory_space=pltpu.SMEM)] + [in_vmem()] * 6,
        out_specs=[in_vmem()] * 3,
        out_shape=[half, half, jax.ShapeDtypeStruct((team, 2 * sources // team, dim), BF16)],
        scratch_shapes=[
            pltpu.VMEM((sources, 2 * dim), BF16),
            pltpu.VMEM((sources, 2 * dim), BF16),
            pltpu.VMEM((dim, sources), BF16),
            pltpu.VMEM((2 * dim, targets), BF16),
            pltpu.VMEM((2 * dim, targets), BF16),
            pltpu.VMEM((targets, dim), BF16),
            pltpu.VMEM((targets, dim), BF16),
            pltpu.VMEM((sources, dim), F32),
            pltpu.VMEM((sources, dim), F32),
            pltpu.VMEM((dim, targets), F32),
        ],
        compiler_params=pltpu.CompilerParams(vmem_limit_bytes=VMEM_LIMIT),
        name="attention_backward",
    )(place, main, small, *keyvals)


def added_up(arrived, copies):
    total = jnp.sum(arrived.astype(F32), axis=0).astype(BF16)
    return jnp.broadcast_to(total[None], (copies, *total.shape))


def exchanged(value, axes):
    return lax.all_to_all(value, axes, 0, 0, tiled=True)


def shifted(value, axis, distance):
    size = lax.axis_size(axis)
    return lax.ppermute(value, axis, [((i + distance) % size, i) for i in range(size)])


def swapped(value, axis, distance):
    pairs = [(i, i ^ distance) for i in range(lax.axis_size(axis))]
    return lax.ppermute(value, axis, pairs)


def summed_to_owner(send, keep):
    distance = 1
    while True:
        arrived = swapped(send, "z", distance)
        total = keep.astype(F32) + arrived.astype(F32)
        count = total.shape[0] // 2
        if count == 0:
            return total[0]
        total = total.astype(BF16)
        keep, send = (total[:count], total[count:])
        distance *= 2


def shards(
    queries, attn_out, out_grad, row_lse, source, saved_keys, saved_values, key_weight, value_weight
):
    src = source.shape[0]
    tp_count = SPLIT[2] * SPLIT[3] * SPLIT[4]
    sp_count = SPLIT[0] * SPLIT[1]
    weight_scale = 1.0 / math.sqrt(src * sp_count)
    main, small, keyvals = pack_rows(
        queries, attn_out, out_grad, row_lse, saved_keys, saved_values
    )
    small = exchanged(small, "z")
    keyvals = [keyvals] + [shifted(keyvals, "y", d) for d in range(1, SPLIT[1])]
    main = lax.all_gather(main, "z", axis=0, tiled=False)
    place = jnp.stack([lax.axis_index("z"), lax.axis_index("y")])
    dq_send, dq_keep, dkv = attention_backward(place, main, small, keyvals)

    dkv = exchanged(dkv, TEAM)
    halves = added_up(dkv, tp_count)
    halves = exchanged(halves, TP).reshape(2, tp_count // 2, 2, -1, HEAD_DIM)
    key_half, value_half = (halves[:, :, i].reshape(2, src, HEAD_DIM) for i in range(2))
    query_grad = summed_to_owner(dq_send, dq_keep)
    key_terms = lax.dot_general(
        key_half, source, (((1,), (0,)), ((), ())), preferred_element_type=F32
    )
    key_terms = (key_terms * weight_scale).astype(BF16).reshape(sp_count, -1, source.shape[1])
    key_terms = exchanged(key_terms, SP)
    key_grad = jnp.sum(key_terms.astype(F32), axis=0)
    weights = jnp.concatenate([key_weight, value_weight], axis=1)
    source_grad = lax.dot_general(
        jnp.concatenate([key_half[0], key_half[1], value_half[0], value_half[1]], axis=1),
        weights,
        (((1,), (1,)), ((), ())),
        preferred_element_type=F32,
    )
    return (query_grad, source_grad, key_grad)


def solution(mesh):
    split = Mesh(mesh.devices.reshape(SPLIT), ("z", "y", "g", "h", "c"))
    return jax.shard_map(
        shards,
        mesh=split,
        in_specs=(
            P(SP, TP),
            P(SP, TP),
            P(SP, TP),
            P(SP, TP),
            P(SP, TP),
            P(SP, None),
            P(SP, None),
            P(TP, None),
            P(TP, None),
        ),
        out_specs=(P(SP, TP), P(SP, TP), P(SP, TP)),
        check_vma=False,
    )
```

```python
import math

import jax
import jax.numpy as jnp
from jax import lax
from jax.experimental import pallas as pl
from jax.experimental.pallas import tpu as pltpu
from jax.sharding import Mesh
from jax.sharding import PartitionSpec as P


HEAD_DIM = 128
SP = ("z", "y")
TP = ("g", "h", "c")
TEAM = ("y", "h", "c")
SPLIT = (16, 4, 2, 2, 2)
F32 = jnp.float32
BF16 = jnp.bfloat16
FIRST = 96
STAT_ROWS = 16
VMEM_LIMIT = 56 * 2**20


def in_vmem():
    return pl.BlockSpec(memory_space=pltpu.VMEM)


def pieces(value):
    high = value.astype(BF16)
    rest = value - high.astype(F32)
    middle = rest.astype(BF16)
    low = (rest - middle.astype(F32)).astype(BF16)
    return [high, middle, low]


def pack_rows(queries, attn_out, out_grad, row_lse, saved_keys, saved_values):
    rows, width = queries.shape
    src = saved_keys.shape[0]
    z_count, y_count = (SPLIT[0], SPLIT[1])

    def kernel(head_ref, q_ref, o_ref, do_ref, lse_ref, k_ref, v_ref, main_ref, last_ref, kv_ref):
        second = head_ref[0] > 0
        main_ref[:rows, :] = q_ref[...]
        main_ref[rows : rows + FIRST, :] = do_ref[:FIRST, :]
        product = do_ref[...].astype(F32) * o_ref[...].astype(F32)
        delta = jnp.sum(product.T, axis=0, keepdims=True)
        stats = pieces(lse_ref[...] * math.sqrt(HEAD_DIM)) + pieces(delta)
        line = lax.broadcasted_iota(jnp.int32, (STAT_ROWS, rows), 0)
        block = jnp.zeros((STAT_ROWS, rows), F32)
        for i, s in enumerate(stats):
            block = jnp.where(line == i, s.astype(F32), block)
        main_ref[rows + FIRST :, :] = block.astype(BF16)
        last = do_ref[FIRST:, :]
        for z in range(z_count):
            last_ref[z] = last
        k = jnp.where(second, k_ref[:, HEAD_DIM:], k_ref[:, :HEAD_DIM])
        v = jnp.where(second, v_ref[:, HEAD_DIM:], v_ref[:, :HEAD_DIM])
        for y in range(y_count):
            kv_ref[y, :src, :] = k
            kv_ref[y, src:, :] = v

    return pl.pallas_call(
        kernel,
        in_specs=[pl.BlockSpec(memory_space=pltpu.SMEM)] + [in_vmem()] * 6,
        out_specs=[in_vmem()] * 3,
        out_shape=[
            jax.ShapeDtypeStruct((rows + FIRST + STAT_ROWS, width), BF16),
            jax.ShapeDtypeStruct((z_count, rows - FIRST, width), BF16),
            jax.ShapeDtypeStruct((y_count, 2 * src, HEAD_DIM), BF16),
        ],
        name="pack_rows",
    )(
        lax.axis_index("g").reshape(1),
        queries,
        attn_out,
        out_grad,
        row_lse.reshape(1, rows),
        saved_keys,
        saved_values,
    )


def dot(left, right):
    return jnp.dot(left, right, preferred_element_type=F32)


def attention_backward(main, keyvals, last=None, before=None, me=None):
    z_count, main_rows, dim = main.shape
    y_count, src = (keyvals.shape[0], keyvals.shape[1] // 2)
    rows = main_rows - FIRST - STAT_ROWS
    low, high = (0, FIRST) if last is None else (FIRST, rows)
    each = high - low
    sources, targets = (y_count * src, z_count * each)
    scale = 1.0 / math.sqrt(HEAD_DIM)
    exp_scale = math.log2(math.e) * scale
    src_tile, tgt_tile = (512, 512)
    team = y_count * SPLIT[3] * SPLIT[4]
    piece = sources // team
    bits = z_count.bit_length() - 1

    def prepare(main_ref, kv_ref, last_ref, k_wide, v_wide, k_turned, q_turned, do_turned, q_rows, do_rows):
        lane = lax.broadcasted_iota(jnp.int32, (src, dim), 1)
        lse_lanes = jnp.where(lane < 3, -1.0, 0.0).astype(BF16)
        delta_lanes = jnp.where((lane >= 3) & (lane < 6), -1.0, 0.0).astype(BF16)
        for y in range(y_count):
            at = slice(y * src, (y + 1) * src)
            k = kv_ref[y, :src, :]
            k_wide[at, :dim] = k
            k_wide[at, dim:] = lse_lanes
            v_wide[at, :dim] = kv_ref[y, src:, :]
            v_wide[at, dim:] = delta_lanes
            k_turned[:, at] = k.T
        blank = jnp.zeros((dim - STAT_ROWS, dim), BF16)
        for z in range(z_count):
            at = slice(z * each, (z + 1) * each)
            q_rows[at, :dim] = main_ref[z, low:high, :]
            stats = jnp.concatenate([main_ref[z, rows + FIRST :, :], blank], axis=0)
            q_rows[at, dim:] = stats.T[low:high, :]
            do_rows[at, :] = main_ref[z, rows : rows + FIRST, :] if last_ref is None else last_ref[z]
        for b in range(0, targets, dim):
            at = slice(b, b + dim)
            q_turned[:dim, at] = q_rows[at, :dim].T
            stats = q_rows[at, dim:].T
            q_turned[dim:, at] = stats
            do_turned[:dim, at] = do_rows[at, :].T
            do_turned[dim:, at] = stats

    def work(k_wide, v_wide, k_turned, q_turned, do_turned, q_rows, do_rows, dk_acc, dv_acc, dq_acc):
        def step(i, carry):
            s = pl.ds(pl.multiple_of(i * src_tile, src_tile), src_tile)
            for t0 in range(0, targets, tgt_tile):
                t = slice(t0, t0 + tgt_tile)
                scores = dot(k_wide[s, :], q_turned[:, t])
                dprobs = dot(v_wide[s, :], do_turned[:, t])
                probs = jnp.exp2(scores * exp_scale)
                dscores = (probs * dprobs).astype(BF16)
                dv_acc[s, :] += dot(probs.astype(BF16), do_rows[t, :])
                dk_acc[s, :] += dot(dscores, q_rows[t, :dim])
                dq_acc[:, t] += dot(k_turned[:, s], dscores)
            return carry

        dq_acc[...] = jnp.zeros_like(dq_acc)
        lax.fori_loop(0, sources // src_tile, step, 0)

    def first_kernel(main_ref, kv_ref, dk_ref, dv_ref, dq_ref, *scratch):
        prepare(main_ref, kv_ref, None, *scratch[:-1])
        dk_ref[...] = jnp.zeros_like(dk_ref)
        dv_ref[...] = jnp.zeros_like(dv_ref)
        work(*scratch[:-1], dk_ref, dv_ref, scratch[-1])
        for z in range(z_count // 4):
            at = slice(z * 4 * each, (z + 1) * 4 * each)
            turned = (scratch[-1][:, at] * scale).T.astype(BF16)
            for i in range(4):
                dq_ref[z * 4 + i] = turned[i * each : (i + 1) * each, :]

    def last_kernel(
        me_ref, main_ref, kv_ref, last_ref, dk_in, dv_in, dq_in, send_ref, keep_ref, dkv_ref, *scratch
    ):
        prepare(main_ref, kv_ref, last_ref, *scratch[:-4])
        dk_acc, dv_acc, dq_acc, dq_rows = scratch[-4:]
        dk_acc[...] = dk_in[...]
        dv_acc[...] = dv_in[...]
        work(*scratch[:-4], dk_acc, dv_acc, dq_acc)
        for i in range(team):
            at = slice(i * piece, (i + 1) * piece)
            dkv_ref[i, :piece, :] = (dk_acc[at, :] * scale).astype(BF16)
            dkv_ref[i, piece:, :] = dv_acc[at, :].astype(BF16)
        for z in range(z_count // 4):
            at = slice(z * 4 * each, (z + 1) * 4 * each)
            turned = (dq_acc[:, at] * scale).T.astype(BF16)
            for i in range(4):
                dq_rows[z * 4 + i] = turned[i * each : (i + 1) * each, :]
        for p in range(z_count):
            turned = sum(((p >> b) & 1) << (bits - 1 - b) for b in range(bits))
            z = jnp.bitwise_xor(me_ref[0], turned)
            out = keep_ref if p < z_count // 2 else send_ref
            out[p % (z_count // 2), :FIRST, :] = dq_in[z]
            out[p % (z_count // 2), FIRST:, :] = dq_rows[z]

    sums = jax.ShapeDtypeStruct((sources, dim), F32)
    scratch = [
        pltpu.VMEM((sources, 2 * dim), BF16),
        pltpu.VMEM((sources, 2 * dim), BF16),
        pltpu.VMEM((dim, sources), BF16),
        pltpu.VMEM((2 * dim, targets), BF16),
        pltpu.VMEM((2 * dim, targets), BF16),
        pltpu.VMEM((targets, 2 * dim), BF16),
        pltpu.VMEM((targets, dim), BF16),
    ]
    params = pltpu.CompilerParams(vmem_limit_bytes=VMEM_LIMIT)
    if last is None:
        return pl.pallas_call(
            first_kernel,
            in_specs=[in_vmem()] * 2,
            out_specs=[in_vmem()] * 3,
            out_shape=[sums, sums, jax.ShapeDtypeStruct((z_count, each, dim), BF16)],
            scratch_shapes=scratch + [pltpu.VMEM((dim, targets), F32)],
            compiler_params=params,
            name="attention_first",
        )(main, keyvals)
    half = jax.ShapeDtypeStruct((z_count // 2, rows, dim), BF16)
    return pl.pallas_call(
        last_kernel,
        in_specs=[pl.BlockSpec(memory_space=pltpu.SMEM)] + [in_vmem()] * 6,
        out_specs=[in_vmem()] * 3,
        out_shape=[half, half, jax.ShapeDtypeStruct((team, 2 * piece, dim), BF16)],
        scratch_shapes=scratch
        + [
            pltpu.VMEM((sources, dim), F32),
            pltpu.VMEM((sources, dim), F32),
            pltpu.VMEM((dim, targets), F32),
            pltpu.VMEM((z_count, each, dim), BF16),
        ],
        compiler_params=params,
        name="attention_last",
    )(me, main, keyvals, last, *before)


def added_up(arrived, copies):
    total = jnp.sum(arrived.astype(F32), axis=0).astype(BF16)
    return jnp.broadcast_to(total[None], (copies, *total.shape))


def exchanged(value, axes):
    return lax.all_to_all(value, axes, 0, 0, tiled=True)


def swapped(value, axis, distance):
    pairs = [(i, i ^ distance) for i in range(lax.axis_size(axis))]
    return lax.ppermute(value, axis, pairs)


def summed_to_owner(send, keep):
    distance = 1
    while True:
        arrived = swapped(send, "z", distance)
        total = keep.astype(F32) + arrived.astype(F32)
        count = total.shape[0] // 2
        if count == 0:
            return total[0]
        total = total.astype(BF16)
        keep, send = (total[:count], total[count:])
        distance *= 2


def shards(
    queries, attn_out, out_grad, row_lse, source, saved_keys, saved_values, key_weight, value_weight
):
    src = source.shape[0]
    tp_count = SPLIT[2] * SPLIT[3] * SPLIT[4]
    sp_count = SPLIT[0] * SPLIT[1]
    weight_scale = 1.0 / math.sqrt(src * sp_count)
    main, last, keyvals = pack_rows(
        queries, attn_out, out_grad, row_lse, saved_keys, saved_values
    )
    keyvals = exchanged(keyvals, "y")
    main = lax.all_gather(main, "z", axis=0, tiled=False)
    last = exchanged(last, "z")
    before = attention_backward(main, keyvals)
    me = lax.axis_index("z").reshape(1)
    dq_send, dq_keep, dkv = attention_backward(main, keyvals, last, before, me)

    dkv = exchanged(dkv, TEAM)
    halves = added_up(dkv, tp_count)
    halves = exchanged(halves, TP).reshape(2, tp_count // 2, 2, -1, HEAD_DIM)
    key_half, value_half = (halves[:, :, i].reshape(2, src, HEAD_DIM) for i in range(2))
    query_grad = summed_to_owner(dq_send, dq_keep)
    key_terms = lax.dot_general(
        key_half, source, (((1,), (0,)), ((), ())), preferred_element_type=F32
    )
    key_terms = (key_terms * weight_scale).astype(BF16).reshape(sp_count, -1, source.shape[1])
    key_terms = exchanged(key_terms, SP)
    key_grad = jnp.sum(key_terms.astype(F32), axis=0)
    weights = jnp.concatenate([key_weight, value_weight], axis=1)
    source_grad = lax.dot_general(
        jnp.concatenate([key_half[0], key_half[1], value_half[0], value_half[1]], axis=1),
        weights,
        (((1,), (1,)), ((), ())),
        preferred_element_type=F32,
    )
    return (query_grad, source_grad, key_grad)


def solution(mesh):
    split = Mesh(mesh.devices.reshape(SPLIT), ("z", "y", "g", "h", "c"))
    return jax.shard_map(
        shards,
        mesh=split,
        in_specs=(
            P(SP, TP),
            P(SP, TP),
            P(SP, TP),
            P(SP, TP),
            P(SP, TP),
            P(SP, None),
            P(SP, None),
            P(TP, None),
            P(TP, None),
        ),
        out_specs=(P(SP, TP), P(SP, TP), P(SP, TP)),
        check_vma=False,
    )
```

```python
import math

import jax
import jax.numpy as jnp
from jax import lax
from jax.experimental import pallas as pl
from jax.experimental.pallas import tpu as pltpu
from jax.sharding import Mesh
from jax.sharding import PartitionSpec as P


HEAD_DIM = 128
SP = ("z", "y")
TP = ("g", "h", "c")
TEAM = ("y", "h", "c")
SPLIT = (16, 4, 2, 2, 2)
F32 = jnp.float32
BF16 = jnp.bfloat16
FIRST = 96
STAT_ROWS = 16
VMEM_LIMIT = 18 * 2**20
PACK_VMEM_LIMIT = 8 * 2**20


def in_vmem():
    return pl.BlockSpec(memory_space=pltpu.VMEM)


def pieces(value):
    high = value.astype(BF16)
    rest = value - high.astype(F32)
    middle = rest.astype(BF16)
    low = (rest - middle.astype(F32)).astype(BF16)
    return [high, middle, low]


def pack_rows(queries, attn_out, out_grad, row_lse, saved_keys, saved_values):
    rows, width = queries.shape
    src = saved_keys.shape[0]
    z_count, y_count = (SPLIT[0], SPLIT[1])

    def kernel(head_ref, q_ref, o_ref, do_ref, lse_ref, k_ref, v_ref, main_ref, last_ref, kv_ref):
        second = head_ref[0] > 0
        main_ref[:rows, :] = q_ref[...]
        main_ref[rows : rows + FIRST, :] = do_ref[:FIRST, :]
        product = do_ref[...].astype(F32) * o_ref[...].astype(F32)
        delta = jnp.sum(product.T, axis=0, keepdims=True)
        stats = pieces(lse_ref[...] * math.sqrt(HEAD_DIM)) + pieces(delta)
        line = lax.broadcasted_iota(jnp.int32, (STAT_ROWS, rows), 0)
        block = jnp.zeros((STAT_ROWS, rows), F32)
        for i, s in enumerate(stats):
            block = jnp.where(line == i, s.astype(F32), block)
        main_ref[rows + FIRST :, :] = block.astype(BF16)
        last = do_ref[FIRST:, :]
        for z in range(z_count):
            last_ref[z] = last
        k = jnp.where(second, k_ref[:, HEAD_DIM:], k_ref[:, :HEAD_DIM])
        v = jnp.where(second, v_ref[:, HEAD_DIM:], v_ref[:, :HEAD_DIM])
        for y in range(y_count):
            kv_ref[y, :src, :] = k
            kv_ref[y, src:, :] = v

    return pl.pallas_call(
        kernel,
        in_specs=[pl.BlockSpec(memory_space=pltpu.SMEM)] + [in_vmem()] * 6,
        out_specs=[in_vmem()] * 3,
        out_shape=[
            jax.ShapeDtypeStruct((rows + FIRST + STAT_ROWS, width), BF16),
            jax.ShapeDtypeStruct((z_count, rows - FIRST, width), BF16),
            jax.ShapeDtypeStruct((y_count, 2 * src, HEAD_DIM), BF16),
        ],
        compiler_params=pltpu.CompilerParams(vmem_limit_bytes=PACK_VMEM_LIMIT),
        name="pack_rows",
    )(
        lax.axis_index("g").reshape(1),
        queries,
        attn_out,
        out_grad,
        row_lse.reshape(1, rows),
        saved_keys,
        saved_values,
    )


def dot(left, right):
    return jnp.dot(left, right, preferred_element_type=F32)


def attention_backward(main, keyvals, last=None, before=None, me=None):
    z_count, main_rows, dim = main.shape
    y_count, src = (keyvals.shape[0], keyvals.shape[1] // 2)
    rows = main_rows - FIRST - STAT_ROWS
    low, high = (0, FIRST) if last is None else (FIRST, rows)
    each = high - low
    sources, targets = (y_count * src, z_count * each)
    scale = 1.0 / math.sqrt(HEAD_DIM)
    exp_scale = math.log2(math.e) * scale
    src_tile, tgt_tile = (512, 512)
    team = y_count * SPLIT[3] * SPLIT[4]
    piece = sources // team
    bits = z_count.bit_length() - 1

    def prepare(main_ref, kv_ref, last_ref, k_wide, v_wide, k_turned, q_turned, do_turned, q_rows, do_rows):
        lane = lax.broadcasted_iota(jnp.int32, (src, dim), 1)
        lse_lanes = jnp.where(lane < 3, -1.0, 0.0).astype(BF16)
        delta_lanes = jnp.where((lane >= 3) & (lane < 6), -1.0, 0.0).astype(BF16)
        for y in range(y_count):
            at = slice(y * src, (y + 1) * src)
            k = kv_ref[y, :src, :]
            k_wide[at, :dim] = k
            k_wide[at, dim:] = lse_lanes
            v_wide[at, :dim] = kv_ref[y, src:, :]
            v_wide[at, dim:] = delta_lanes
            k_turned[:, at] = k.T
        blank = jnp.zeros((dim - STAT_ROWS, dim), BF16)
        for z in range(z_count):
            at = slice(z * each, (z + 1) * each)
            q_rows[at, :dim] = main_ref[z, low:high, :]
            stats = jnp.concatenate([main_ref[z, rows + FIRST :, :], blank], axis=0)
            q_rows[at, dim:] = stats.T[low:high, :]
            do_rows[at, :] = main_ref[z, rows : rows + FIRST, :] if last_ref is None else last_ref[z]
        for b in range(0, targets, dim):
            at = slice(b, b + dim)
            q_turned[:dim, at] = q_rows[at, :dim].T
            stats = q_rows[at, dim:].T
            q_turned[dim:, at] = stats
            do_turned[:dim, at] = do_rows[at, :].T
            do_turned[dim:, at] = stats

    def work(k_wide, v_wide, k_turned, q_turned, do_turned, q_rows, do_rows, dk_acc, dv_acc, dq_acc):
        def step(i, carry):
            s = pl.ds(pl.multiple_of(i * src_tile, src_tile), src_tile)
            for t0 in range(0, targets, tgt_tile):
                t = slice(t0, t0 + tgt_tile)
                scores = dot(k_wide[s, :], q_turned[:, t])
                dprobs = dot(v_wide[s, :], do_turned[:, t])
                probs = jnp.exp2(scores * exp_scale)
                dscores = (probs * dprobs).astype(BF16)
                dv_acc[s, :] += dot(probs.astype(BF16), do_rows[t, :])
                dk_acc[s, :] += dot(dscores, q_rows[t, :dim])
                dq_acc[:, t] += dot(k_turned[:, s], dscores)
            return carry

        dq_acc[...] = jnp.zeros_like(dq_acc)
        lax.fori_loop(0, sources // src_tile, step, 0)

    def first_kernel(main_ref, kv_ref, dk_ref, dv_ref, dq_ref, *scratch):
        prepare(main_ref, kv_ref, None, *scratch[:-1])
        dk_ref[...] = jnp.zeros_like(dk_ref)
        dv_ref[...] = jnp.zeros_like(dv_ref)
        work(*scratch[:-1], dk_ref, dv_ref, scratch[-1])
        for z in range(z_count // 4):
            at = slice(z * 4 * each, (z + 1) * 4 * each)
            turned = (scratch[-1][:, at] * scale).T.astype(BF16)
            for i in range(4):
                dq_ref[z * 4 + i] = turned[i * each : (i + 1) * each, :]

    def last_kernel(
        me_ref, main_ref, kv_ref, last_ref, dk_in, dv_in, dq_in, send_ref, keep_ref, dkv_ref, *scratch
    ):
        prepare(main_ref, kv_ref, last_ref, *scratch[:-4])
        dk_acc, dv_acc, dq_acc, dq_rows = scratch[-4:]
        dk_acc[...] = dk_in[...]
        dv_acc[...] = dv_in[...]
        work(*scratch[:-4], dk_acc, dv_acc, dq_acc)
        for i in range(team):
            at = slice(i * piece, (i + 1) * piece)
            dkv_ref[i, :piece, :] = (dk_acc[at, :] * scale).astype(BF16)
            dkv_ref[i, piece:, :] = dv_acc[at, :].astype(BF16)
        for z in range(z_count // 4):
            at = slice(z * 4 * each, (z + 1) * 4 * each)
            turned = (dq_acc[:, at] * scale).T.astype(BF16)
            for i in range(4):
                dq_rows[z * 4 + i] = turned[i * each : (i + 1) * each, :]
        for p in range(z_count):
            turned = sum(((p >> b) & 1) << (bits - 1 - b) for b in range(bits))
            z = jnp.bitwise_xor(me_ref[0], turned)
            out = keep_ref if p < z_count // 2 else send_ref
            out[p % (z_count // 2), :FIRST, :] = dq_in[z]
            out[p % (z_count // 2), FIRST:, :] = dq_rows[z]

    sums = jax.ShapeDtypeStruct((sources, dim), F32)
    scratch = [
        pltpu.VMEM((sources, 2 * dim), BF16),
        pltpu.VMEM((sources, 2 * dim), BF16),
        pltpu.VMEM((dim, sources), BF16),
        pltpu.VMEM((2 * dim, targets), BF16),
        pltpu.VMEM((2 * dim, targets), BF16),
        pltpu.VMEM((targets, 2 * dim), BF16),
        pltpu.VMEM((targets, dim), BF16),
    ]
    params = pltpu.CompilerParams(vmem_limit_bytes=VMEM_LIMIT)
    if last is None:
        return pl.pallas_call(
            first_kernel,
            in_specs=[in_vmem()] * 2,
            out_specs=[in_vmem()] * 3,
            out_shape=[sums, sums, jax.ShapeDtypeStruct((z_count, each, dim), BF16)],
            scratch_shapes=scratch + [pltpu.VMEM((dim, targets), F32)],
            compiler_params=params,
            name="attention_first",
        )(main, keyvals)
    half = jax.ShapeDtypeStruct((z_count // 2, rows, dim), BF16)
    return pl.pallas_call(
        last_kernel,
        in_specs=[pl.BlockSpec(memory_space=pltpu.SMEM)] + [in_vmem()] * 6,
        out_specs=[in_vmem()] * 3,
        out_shape=[half, half, jax.ShapeDtypeStruct((team, 2 * piece, dim), BF16)],
        scratch_shapes=scratch
        + [
            pltpu.VMEM((sources, dim), F32),
            pltpu.VMEM((sources, dim), F32),
            pltpu.VMEM((dim, targets), F32),
            pltpu.VMEM((z_count, each, dim), BF16),
        ],
        compiler_params=params,
        name="attention_last",
    )(me, main, keyvals, last, *before)


def added_up(arrived, copies):
    total = jnp.sum(arrived.astype(F32), axis=0).astype(BF16)
    return jnp.broadcast_to(total[None], (copies, *total.shape))


def exchanged(value, axes):
    return lax.all_to_all(value, axes, 0, 0, tiled=True)


def swapped(value, axis, distance):
    pairs = [(i, i ^ distance) for i in range(lax.axis_size(axis))]
    return lax.ppermute(value, axis, pairs)


def summed_to_owner(send, keep):
    distance = 1
    while True:
        arrived = swapped(send, "z", distance)
        count = keep.shape[0] // 2
        if count == 0:
            return keep[0].astype(F32) + arrived[0].astype(F32)
        send = (keep[count:].astype(F32) + arrived[count:].astype(F32)).astype(BF16)
        keep, arrived = lax.optimization_barrier((keep, arrived))
        keep = (keep[:count].astype(F32) + arrived[:count].astype(F32)).astype(BF16)
        distance *= 2


def shards(
    queries, attn_out, out_grad, row_lse, source, saved_keys, saved_values, key_weight, value_weight
):
    src = source.shape[0]
    tp_count = SPLIT[2] * SPLIT[3] * SPLIT[4]
    sp_count = SPLIT[0] * SPLIT[1]
    weight_scale = 1.0 / math.sqrt(src * sp_count)
    main, last, keyvals = pack_rows(
        queries, attn_out, out_grad, row_lse, saved_keys, saved_values
    )
    keyvals = exchanged(keyvals, "y")
    main = lax.all_gather(main, "z", axis=0, tiled=False)
    last = exchanged(last, "z")
    before = attention_backward(main, keyvals)
    me = lax.axis_index("z").reshape(1)
    dq_send, dq_keep, dkv = attention_backward(main, keyvals, last, before, me)

    dkv = exchanged(dkv, TEAM)
    halves = added_up(dkv, tp_count)
    halves = exchanged(halves, TP).reshape(2, tp_count // 2, 2, -1, HEAD_DIM)
    key_half, value_half = (halves[:, :, i].reshape(2, src, HEAD_DIM) for i in range(2))
    query_grad = summed_to_owner(dq_send, dq_keep)
    key_terms = lax.dot_general(
        key_half, source, (((1,), (0,)), ((), ())), preferred_element_type=F32
    )
    key_terms = (key_terms * weight_scale).astype(BF16).reshape(sp_count, -1, source.shape[1])
    key_terms = exchanged(key_terms, SP)
    key_grad = jnp.sum(key_terms.astype(F32), axis=0)
    weights = jnp.concatenate([key_weight, value_weight], axis=1)
    source_grad = lax.dot_general(
        jnp.concatenate([key_half[0], key_half[1], value_half[0], value_half[1]], axis=1),
        weights,
        (((1,), (1,)), ((), ())),
        preferred_element_type=F32,
    )
    return (query_grad, source_grad, key_grad)


def solution(mesh):
    split = Mesh(mesh.devices.reshape(SPLIT), ("z", "y", "g", "h", "c"))
    return jax.shard_map(
        shards,
        mesh=split,
        in_specs=(
            P(SP, TP),
            P(SP, TP),
            P(SP, TP),
            P(SP, TP),
            P(SP, TP),
            P(SP, None),
            P(SP, None),
            P(TP, None),
            P(TP, None),
        ),
        out_specs=(P(SP, TP), P(SP, TP), P(SP, TP)),
        check_vma=False,
    )
```

```python
import math

import jax
import jax.numpy as jnp
from jax import lax
from jax.experimental import pallas as pl
from jax.experimental.pallas import tpu as pltpu
from jax.sharding import Mesh
from jax.sharding import PartitionSpec as P


HEAD_DIM = 128
SP = ("z", "y")
TP = ("g", "h", "c")
TEAM = ("y", "h", "c")
SPLIT = (16, 4, 2, 2, 2)
F32 = jnp.float32
BF16 = jnp.bfloat16
FIRST = 96
STAT_ROWS = 16
FIRST_VMEM_LIMIT = 18 * 2**20
LAST_VMEM_LIMIT = 56 * 2**20


def in_vmem():
    return pl.BlockSpec(memory_space=pltpu.VMEM)


def pieces(value):
    high = value.astype(BF16)
    rest = value - high.astype(F32)
    middle = rest.astype(BF16)
    low = (rest - middle.astype(F32)).astype(BF16)
    return [high, middle, low]


def pack_rows(queries, attn_out, out_grad, row_lse, saved_keys, saved_values):
    rows, width = queries.shape
    src = saved_keys.shape[0]
    z_count, y_count = (SPLIT[0], SPLIT[1])

    def kernel(head_ref, q_ref, o_ref, do_ref, lse_ref, k_ref, v_ref, main_ref, last_ref, kv_ref):
        second = head_ref[0] > 0
        main_ref[:rows, :] = q_ref[...]
        main_ref[rows : rows + FIRST, :] = do_ref[:FIRST, :]
        product = do_ref[...].astype(F32) * o_ref[...].astype(F32)
        delta = jnp.sum(product.T, axis=0, keepdims=True)
        stats = pieces(lse_ref[...] * math.sqrt(HEAD_DIM)) + pieces(delta)
        line = lax.broadcasted_iota(jnp.int32, (STAT_ROWS, rows), 0)
        block = jnp.zeros((STAT_ROWS, rows), F32)
        for i, s in enumerate(stats):
            block = jnp.where(line == i, s.astype(F32), block)
        main_ref[rows + FIRST :, :] = block.astype(BF16)
        last = do_ref[FIRST:, :]
        for z in range(z_count):
            last_ref[z] = last
        k = jnp.where(second, k_ref[:, HEAD_DIM:], k_ref[:, :HEAD_DIM])
        v = jnp.where(second, v_ref[:, HEAD_DIM:], v_ref[:, :HEAD_DIM])
        for y in range(y_count):
            kv_ref[y, :src, :] = k
            kv_ref[y, src:, :] = v

    return pl.pallas_call(
        kernel,
        in_specs=[pl.BlockSpec(memory_space=pltpu.SMEM)] + [in_vmem()] * 6,
        out_specs=[in_vmem()] * 3,
        out_shape=[
            jax.ShapeDtypeStruct((rows + FIRST + STAT_ROWS, width), BF16),
            jax.ShapeDtypeStruct((z_count, rows - FIRST, width), BF16),
            jax.ShapeDtypeStruct((y_count, 2 * src, HEAD_DIM), BF16),
        ],
        name="pack_rows",
    )(
        lax.axis_index("g").reshape(1),
        queries,
        attn_out,
        out_grad,
        row_lse.reshape(1, rows),
        saved_keys,
        saved_values,
    )


def dot(left, right):
    return jnp.dot(left, right, preferred_element_type=F32)


def attention_backward(main, keyvals, last=None, before=None, me=None):
    z_count, main_rows, dim = main.shape
    y_count, src = (keyvals.shape[0], keyvals.shape[1] // 2)
    rows = main_rows - FIRST - STAT_ROWS
    low, high = (0, FIRST) if last is None else (FIRST, rows)
    each = high - low
    sources, targets = (y_count * src, z_count * each)
    scale = 1.0 / math.sqrt(HEAD_DIM)
    exp_scale = math.log2(math.e) * scale
    src_tile, tgt_tile = (512, 512)
    team = y_count * SPLIT[3] * SPLIT[4]
    piece = sources // team
    bits = z_count.bit_length() - 1

    def prepare(main_ref, kv_ref, last_ref, k_wide, v_wide, k_turned, q_turned, do_turned, q_rows, do_rows):
        lane = lax.broadcasted_iota(jnp.int32, (src, dim), 1)
        lse_lanes = jnp.where(lane < 3, -1.0, 0.0).astype(BF16)
        delta_lanes = jnp.where((lane >= 3) & (lane < 6), -1.0, 0.0).astype(BF16)
        for y in range(y_count):
            at = slice(y * src, (y + 1) * src)
            k = kv_ref[y, :src, :]
            k_wide[at, :dim] = k
            k_wide[at, dim:] = lse_lanes
            v_wide[at, :dim] = kv_ref[y, src:, :]
            v_wide[at, dim:] = delta_lanes
            k_turned[:, at] = k.T
        blank = jnp.zeros((dim - STAT_ROWS, dim), BF16)
        for z in range(z_count):
            at = slice(z * each, (z + 1) * each)
            q_rows[at, :dim] = main_ref[z, low:high, :]
            stats = jnp.concatenate([main_ref[z, rows + FIRST :, :], blank], axis=0)
            q_rows[at, dim:] = stats.T[low:high, :]
            do_rows[at, :] = main_ref[z, rows : rows + FIRST, :] if last_ref is None else last_ref[z]
        for b in range(0, targets, dim):
            at = slice(b, b + dim)
            q_turned[:dim, at] = q_rows[at, :dim].T
            stats = q_rows[at, dim:].T
            q_turned[dim:, at] = stats
            do_turned[:dim, at] = do_rows[at, :].T
            do_turned[dim:, at] = stats

    def work(k_wide, v_wide, k_turned, q_turned, do_turned, q_rows, do_rows, dk_acc, dv_acc, dq_acc):
        def step(i, carry):
            s = pl.ds(pl.multiple_of(i * src_tile, src_tile), src_tile)
            for t0 in range(0, targets, tgt_tile):
                t = slice(t0, t0 + tgt_tile)
                scores = dot(k_wide[s, :], q_turned[:, t])
                dprobs = dot(v_wide[s, :], do_turned[:, t])
                probs = jnp.exp2(scores * exp_scale)
                dscores = (probs * dprobs).astype(BF16)
                dv_acc[s, :] += dot(probs.astype(BF16), do_rows[t, :])
                dk_acc[s, :] += dot(dscores, q_rows[t, :dim])
                dq_acc[:, t] += dot(k_turned[:, s], dscores)
            return carry

        dk_acc[...] = jnp.zeros_like(dk_acc)
        dv_acc[...] = jnp.zeros_like(dv_acc)
        dq_acc[...] = jnp.zeros_like(dq_acc)
        lax.fori_loop(0, sources // src_tile, step, 0)

    def first_kernel(main_ref, kv_ref, dkv_ref, dq_ref, *scratch):
        dk_acc, dv_acc, dq_acc = scratch[-3:]
        prepare(main_ref, kv_ref, None, *scratch[:-3])
        work(*scratch)
        for i in range(team):
            at = slice(i * piece, (i + 1) * piece)
            dkv_ref[i, :piece, :] = (dk_acc[at, :] * scale).astype(BF16)
            dkv_ref[i, piece:, :] = dv_acc[at, :].astype(BF16)
        for z in range(z_count // 4):
            at = slice(z * 4 * each, (z + 1) * 4 * each)
            turned = (dq_acc[:, at] * scale).T.astype(BF16)
            for i in range(4):
                dq_ref[z * 4 + i] = turned[i * each : (i + 1) * each, :]

    def last_kernel(
        me_ref, main_ref, kv_ref, last_ref, dkv_in, dq_in, send_ref, keep_ref, dkv_ref, *scratch
    ):
        dk_acc, dv_acc, dq_acc, dq_rows = scratch[-4:]
        prepare(main_ref, kv_ref, last_ref, *scratch[:-4])
        work(*scratch[:-1])
        for i in range(team):
            at = slice(i * piece, (i + 1) * piece)
            dk_before = dkv_in[i, :piece, :].astype(F32)
            dv_before = dkv_in[i, piece:, :].astype(F32)
            dkv_ref[i, :piece, :] = (dk_acc[at, :] * scale + dk_before).astype(BF16)
            dkv_ref[i, piece:, :] = (dv_acc[at, :] + dv_before).astype(BF16)
        for z in range(z_count // 4):
            at = slice(z * 4 * each, (z + 1) * 4 * each)
            turned = (dq_acc[:, at] * scale).T.astype(BF16)
            for i in range(4):
                dq_rows[z * 4 + i] = turned[i * each : (i + 1) * each, :]
        for p in range(z_count):
            turned = sum(((p >> b) & 1) << (bits - 1 - b) for b in range(bits))
            z = jnp.bitwise_xor(me_ref[0], turned)
            out = keep_ref if p < z_count // 2 else send_ref
            out[p % (z_count // 2), :FIRST, :] = dq_in[z]
            out[p % (z_count // 2), FIRST:, :] = dq_rows[z]

    dkv = jax.ShapeDtypeStruct((team, 2 * piece, dim), BF16)
    scratch = [
        pltpu.VMEM((sources, 2 * dim), BF16),
        pltpu.VMEM((sources, 2 * dim), BF16),
        pltpu.VMEM((dim, sources), BF16),
        pltpu.VMEM((2 * dim, targets), BF16),
        pltpu.VMEM((2 * dim, targets), BF16),
        pltpu.VMEM((targets, 2 * dim), BF16),
        pltpu.VMEM((targets, dim), BF16),
        pltpu.VMEM((sources, dim), F32),
        pltpu.VMEM((sources, dim), F32),
        pltpu.VMEM((dim, targets), F32),
    ]
    if last is None:
        return pl.pallas_call(
            first_kernel,
            in_specs=[in_vmem()] * 2,
            out_specs=[in_vmem()] * 2,
            out_shape=[dkv, jax.ShapeDtypeStruct((z_count, each, dim), BF16)],
            scratch_shapes=scratch,
            compiler_params=pltpu.CompilerParams(vmem_limit_bytes=FIRST_VMEM_LIMIT),
            name="attention_first",
        )(main, keyvals)
    half = jax.ShapeDtypeStruct((z_count // 2, rows, dim), BF16)
    return pl.pallas_call(
        last_kernel,
        in_specs=[pl.BlockSpec(memory_space=pltpu.SMEM)] + [in_vmem()] * 5,
        out_specs=[in_vmem()] * 3,
        out_shape=[half, half, dkv],
        scratch_shapes=scratch + [pltpu.VMEM((z_count, each, dim), BF16)],
        compiler_params=pltpu.CompilerParams(vmem_limit_bytes=LAST_VMEM_LIMIT),
        name="attention_last",
    )(me, main, keyvals, last, *before)


def added_up(arrived, copies):
    total = jnp.sum(arrived.astype(F32), axis=0).astype(BF16)
    return jnp.broadcast_to(total[None], (copies, *total.shape))


def exchanged(value, axes):
    return lax.all_to_all(value, axes, 0, 0, tiled=True)


def swapped(value, axis, distance):
    pairs = [(i, i ^ distance) for i in range(lax.axis_size(axis))]
    return lax.ppermute(value, axis, pairs)


def summed_to_owner(send, keep):
    for distance in (1, 2):
        arrived = swapped(send, "z", distance)
        count = keep.shape[0] // 2
        send = (keep[count:].astype(F32) + arrived[count:].astype(F32)).astype(BF16)
        if count == 4:
            keep, arrived = lax.optimization_barrier((keep, arrived))
        else:
            middle = (keep[1:2].astype(F32) + arrived[1:2].astype(F32)).astype(BF16)
            keep, arrived = lax.optimization_barrier((keep[:1], arrived[:1]))
        keep = keep[: send.shape[0]].astype(F32) + arrived[: send.shape[0]].astype(F32)
        keep = keep.astype(BF16) if count == 4 else keep[0]
    arrived = [swapped(send[:1], "z", 4), swapped(middle, "z", 8), swapped(send[1:], "z", 12)]
    return keep + sum(a[0].astype(F32) for a in arrived)


def shards(
    queries, attn_out, out_grad, row_lse, source, saved_keys, saved_values, key_weight, value_weight
):
    src = source.shape[0]
    tp_count = SPLIT[2] * SPLIT[3] * SPLIT[4]
    sp_count = SPLIT[0] * SPLIT[1]
    weight_scale = 1.0 / math.sqrt(src * sp_count)
    main, last, keyvals = pack_rows(
        queries, attn_out, out_grad, row_lse, saved_keys, saved_values
    )
    keyvals = exchanged(keyvals, "y")
    main = lax.all_gather(main, "z", axis=0, tiled=False)
    last = exchanged(last, "z")
    before = attention_backward(main, keyvals)
    me = lax.axis_index("z").reshape(1)
    dq_send, dq_keep, dkv = attention_backward(main, keyvals, last, before, me)

    dkv = exchanged(dkv, TEAM)
    halves = added_up(dkv, tp_count)
    halves = exchanged(halves, TP).reshape(2, tp_count // 2, 2, -1, HEAD_DIM)
    key_half, value_half = (halves[:, :, i].reshape(2, src, HEAD_DIM) for i in range(2))
    query_grad = summed_to_owner(dq_send, dq_keep)
    key_terms = lax.dot_general(
        key_half, source, (((1,), (0,)), ((), ())), preferred_element_type=F32
    )
    key_terms = (key_terms * weight_scale).astype(BF16).reshape(sp_count, -1, source.shape[1])
    key_terms = exchanged(key_terms, SP)
    key_grad = jnp.sum(key_terms.astype(F32), axis=0)
    weights = jnp.concatenate([key_weight, value_weight], axis=1)
    source_grad = lax.dot_general(
        jnp.concatenate([key_half[0], key_half[1], value_half[0], value_half[1]], axis=1),
        weights,
        (((1,), (1,)), ((), ())),
        preferred_element_type=F32,
    )
    return (query_grad, source_grad, key_grad)


def solution(mesh):
    split = Mesh(mesh.devices.reshape(SPLIT), ("z", "y", "g", "h", "c"))
    return jax.shard_map(
        shards,
        mesh=split,
        in_specs=(
            P(SP, TP),
            P(SP, TP),
            P(SP, TP),
            P(SP, TP),
            P(SP, TP),
            P(SP, None),
            P(SP, None),
            P(TP, None),
            P(TP, None),
        ),
        out_specs=(P(SP, TP), P(SP, TP), P(SP, TP)),
        check_vma=False,
    )
```

```python
import math

import jax
import jax.numpy as jnp
from jax import lax
from jax.experimental import pallas as pl
from jax.experimental.pallas import tpu as pltpu
from jax.sharding import Mesh
from jax.sharding import PartitionSpec as P


HEAD_DIM = 128
SP = ("z", "y")
TP = ("g", "h", "c")
TEAM = ("y", "h", "c")
SPLIT = (16, 4, 2, 2, 2)
F32 = jnp.float32
BF16 = jnp.bfloat16
FIRST = 96
STAT_ROWS = 16
FIRST_VMEM_LIMIT = 18 * 2**20
LAST_VMEM_LIMIT = 56 * 2**20
SMALL_VMEM_LIMIT = 8 * 2**20


def in_vmem():
    return pl.BlockSpec(memory_space=pltpu.VMEM)


def pieces(value):
    high = value.astype(BF16)
    rest = value - high.astype(F32)
    middle = rest.astype(BF16)
    low = (rest - middle.astype(F32)).astype(BF16)
    return [high, middle, low]


def pack_rows(queries, attn_out, out_grad, row_lse, saved_keys, saved_values):
    rows, width = queries.shape
    src = saved_keys.shape[0]
    z_count, y_count = (SPLIT[0], SPLIT[1])

    def kernel(head_ref, q_ref, o_ref, do_ref, lse_ref, k_ref, v_ref, main_ref, last_ref, kv_ref):
        second = head_ref[0] > 0
        main_ref[:rows, :] = q_ref[...]
        main_ref[rows : rows + FIRST, :] = do_ref[:FIRST, :]
        product = do_ref[...].astype(F32) * o_ref[...].astype(F32)
        delta = jnp.sum(product.T, axis=0, keepdims=True)
        stats = pieces(lse_ref[...] * math.sqrt(HEAD_DIM)) + pieces(delta)
        line = lax.broadcasted_iota(jnp.int32, (STAT_ROWS, rows), 0)
        block = jnp.zeros((STAT_ROWS, rows), F32)
        for i, s in enumerate(stats):
            block = jnp.where(line == i, s.astype(F32), block)
        main_ref[rows + FIRST :, :] = block.astype(BF16)
        last = do_ref[FIRST:, :]
        for z in range(z_count):
            last_ref[z] = last
        k = jnp.where(second, k_ref[:, HEAD_DIM:], k_ref[:, :HEAD_DIM])
        v = jnp.where(second, v_ref[:, HEAD_DIM:], v_ref[:, :HEAD_DIM])
        for y in range(y_count):
            kv_ref[y, :src, :] = k
            kv_ref[y, src:, :] = v

    return pl.pallas_call(
        kernel,
        in_specs=[pl.BlockSpec(memory_space=pltpu.SMEM)] + [in_vmem()] * 6,
        out_specs=[in_vmem()] * 3,
        out_shape=[
            jax.ShapeDtypeStruct((rows + FIRST + STAT_ROWS, width), BF16),
            jax.ShapeDtypeStruct((z_count, rows - FIRST, width), BF16),
            jax.ShapeDtypeStruct((y_count, 2 * src, HEAD_DIM), BF16),
        ],
        name="pack_rows",
    )(
        lax.axis_index("g").reshape(1),
        queries,
        attn_out,
        out_grad,
        row_lse.reshape(1, rows),
        saved_keys,
        saved_values,
    )


def dot(left, right):
    return jnp.dot(left, right, preferred_element_type=F32)


def attention_backward(main, keyvals, last=None, before=None, me=None):
    z_count, main_rows, dim = main.shape
    y_count, src = (keyvals.shape[0], keyvals.shape[1] // 2)
    rows = main_rows - FIRST - STAT_ROWS
    low, high = (0, FIRST) if last is None else (FIRST, rows)
    each = high - low
    sources, targets = (y_count * src, z_count * each)
    scale = 1.0 / math.sqrt(HEAD_DIM)
    exp_scale = math.log2(math.e) * scale
    src_tile, tgt_tile = (512, 512)
    team = y_count * SPLIT[3] * SPLIT[4]
    piece = sources // team

    def prepare(main_ref, kv_ref, last_ref, k_wide, v_wide, k_turned, q_turned, do_turned, q_rows, do_rows):
        lane = lax.broadcasted_iota(jnp.int32, (src, dim), 1)
        lse_lanes = jnp.where(lane < 3, -1.0, 0.0).astype(BF16)
        delta_lanes = jnp.where((lane >= 3) & (lane < 6), -1.0, 0.0).astype(BF16)
        for y in range(y_count):
            at = slice(y * src, (y + 1) * src)
            k = kv_ref[y, :src, :]
            k_wide[at, :dim] = k
            k_wide[at, dim:] = lse_lanes
            v_wide[at, :dim] = kv_ref[y, src:, :]
            v_wide[at, dim:] = delta_lanes
            k_turned[:, at] = k.T
        blank = jnp.zeros((dim - STAT_ROWS, dim), BF16)
        for z in range(z_count):
            at = slice(z * each, (z + 1) * each)
            q_rows[at, :dim] = main_ref[z, low:high, :]
            stats = jnp.concatenate([main_ref[z, rows + FIRST :, :], blank], axis=0)
            q_rows[at, dim:] = stats.T[low:high, :]
            do_rows[at, :] = main_ref[z, rows : rows + FIRST, :] if last_ref is None else last_ref[z]
        for b in range(0, targets, dim):
            at = slice(b, b + dim)
            q_turned[:dim, at] = q_rows[at, :dim].T
            stats = q_rows[at, dim:].T
            q_turned[dim:, at] = stats
            do_turned[:dim, at] = do_rows[at, :].T
            do_turned[dim:, at] = stats

    def work(k_wide, v_wide, k_turned, q_turned, do_turned, q_rows, do_rows, dk_acc, dv_acc, dq_acc):
        def step(i, carry):
            s = pl.ds(pl.multiple_of(i * src_tile, src_tile), src_tile)
            for t0 in range(0, targets, tgt_tile):
                t = slice(t0, t0 + tgt_tile)
                scores = dot(k_wide[s, :], q_turned[:, t])
                dprobs = dot(v_wide[s, :], do_turned[:, t])
                probs = jnp.exp2(scores * exp_scale)
                dscores = (probs * dprobs).astype(BF16)
                dv_acc[s, :] += dot(probs.astype(BF16), do_rows[t, :])
                dk_acc[s, :] += dot(dscores, q_rows[t, :dim])
                dq_acc[:, t] += dot(k_turned[:, s], dscores)
            return carry

        dk_acc[...] = jnp.zeros_like(dk_acc)
        dv_acc[...] = jnp.zeros_like(dv_acc)
        dq_acc[...] = jnp.zeros_like(dq_acc)
        lax.fori_loop(0, sources // src_tile, step, 0)

    def first_kernel(main_ref, kv_ref, dkv_ref, dq_ref, *scratch):
        dk_acc, dv_acc, dq_acc = scratch[-3:]
        prepare(main_ref, kv_ref, None, *scratch[:-3])
        work(*scratch)
        for i in range(team):
            at = slice(i * piece, (i + 1) * piece)
            dkv_ref[i, :piece, :] = (dk_acc[at, :] * scale).astype(BF16)
            dkv_ref[i, piece:, :] = dv_acc[at, :].astype(BF16)
        for z in range(z_count // 4):
            at = slice(z * 4 * each, (z + 1) * 4 * each)
            turned = (dq_acc[:, at] * scale).T.astype(BF16)
            for i in range(4):
                dq_ref[z * 4 + i] = turned[i * each : (i + 1) * each, :]

    def last_kernel(
        me_ref, main_ref, kv_ref, last_ref, dkv_in, dq_in, send_ref, keep_ref, dkv_ref, *scratch
    ):
        dk_acc, dv_acc, dq_acc, dq_rows = scratch[-4:]
        prepare(main_ref, kv_ref, last_ref, *scratch[:-4])
        work(*scratch[:-1])
        for i in range(team):
            at = slice(i * piece, (i + 1) * piece)
            dk_before = dkv_in[i, :piece, :].astype(F32)
            dv_before = dkv_in[i, piece:, :].astype(F32)
            dkv_ref[i, :piece, :] = (dk_acc[at, :] * scale + dk_before).astype(BF16)
            dkv_ref[i, piece:, :] = (dv_acc[at, :] + dv_before).astype(BF16)
        for z in range(z_count // 4):
            at = slice(z * 4 * each, (z + 1) * 4 * each)
            turned = (dq_acc[:, at] * scale).T.astype(BF16)
            for i in range(4):
                dq_rows[z * 4 + i] = turned[i * each : (i + 1) * each, :]
        half_rows = rows // 2
        for odd, (low_ref, high_ref) in enumerate(((keep_ref, send_ref), (send_ref, keep_ref))):

            @pl.when(me_ref[0] == odd)
            def _(low_ref=low_ref, high_ref=high_ref):
                low_ref[...] = dq_in[:, :half_rows, :]
                high_ref[:, : FIRST - half_rows, :] = dq_in[:, half_rows:, :]
                high_ref[:, FIRST - half_rows :, :] = dq_rows[...]

    dkv = jax.ShapeDtypeStruct((team, 2 * piece, dim), BF16)
    scratch = [
        pltpu.VMEM((sources, 2 * dim), BF16),
        pltpu.VMEM((sources, 2 * dim), BF16),
        pltpu.VMEM((dim, sources), BF16),
        pltpu.VMEM((2 * dim, targets), BF16),
        pltpu.VMEM((2 * dim, targets), BF16),
        pltpu.VMEM((targets, 2 * dim), BF16),
        pltpu.VMEM((targets, dim), BF16),
        pltpu.VMEM((sources, dim), F32),
        pltpu.VMEM((sources, dim), F32),
        pltpu.VMEM((dim, targets), F32),
    ]
    if last is None:
        return pl.pallas_call(
            first_kernel,
            in_specs=[in_vmem()] * 2,
            out_specs=[in_vmem()] * 2,
            out_shape=[dkv, jax.ShapeDtypeStruct((z_count, each, dim), BF16)],
            scratch_shapes=scratch,
            compiler_params=pltpu.CompilerParams(vmem_limit_bytes=FIRST_VMEM_LIMIT),
            name="attention_first",
        )(main, keyvals)
    half = jax.ShapeDtypeStruct((z_count, rows // 2, dim), BF16)
    return pl.pallas_call(
        last_kernel,
        in_specs=[pl.BlockSpec(memory_space=pltpu.SMEM)] + [in_vmem()] * 5,
        out_specs=[in_vmem()] * 3,
        out_shape=[half, half, dkv],
        scratch_shapes=scratch + [pltpu.VMEM((z_count, each, dim), BF16)],
        compiler_params=pltpu.CompilerParams(vmem_limit_bytes=LAST_VMEM_LIMIT),
        name="attention_last",
    )(me, main, keyvals, last, *before)


def added_up(arrived, copies):
    total = jnp.sum(arrived.astype(F32), axis=0).astype(BF16)
    return jnp.broadcast_to(total[None], (copies, *total.shape))


def exchanged(value, axes):
    return lax.all_to_all(value, axes, 0, 0, tiled=True)


def swapped(value, axis, distance):
    pairs = [(i, i ^ distance) for i in range(lax.axis_size(axis))]
    return lax.ppermute(value, axis, pairs)


def rows_by_turns(send, keep):
    arrived = swapped(send, "z", 1)
    count = keep.shape[1] // 2
    mine = jnp.bitwise_and(lax.shift_right_logical(lax.axis_index("z"), 1), 1)

    def part(index):
        a, b = (jnp.where(index > 0, v[:, count:], v[:, :count]) for v in (keep, arrived))
        return (a.astype(F32) + b.astype(F32)).astype(BF16)

    send = part(1 - mine)
    keep, arrived = lax.optimization_barrier((keep, arrived))
    keep = part(mine)
    return keep, swapped(send, "z", 2)


def shuffled(value, outer, middle, inner):
    rows = outer * middle * inner
    new = lax.broadcasted_iota(jnp.int32, (rows, rows), 0)
    old = lax.broadcasted_iota(jnp.int32, (rows, rows), 1)
    m, o, i = (new // (outer * inner), new // inner % outer, new % inner)
    take = old == (o * middle + m) * inner + i
    return dot(jnp.where(take, 1.0, 0.0).astype(BF16), value).astype(BF16)


def key_products(halves, source, weight_scale):
    parts, rows, dim = halves.shape
    z_count, y_count = (SPLIT[0], SPLIT[1])
    own = 2 * dim // (z_count * y_count)

    def kernel(halves_ref, source_ref, out_ref):
        terms = []
        for g in range(2):
            key = jnp.concatenate(
                [halves_ref[g * parts // 2 + p, : rows // 2, :] for p in range(parts // 2)], axis=0
            )
            terms.append(dot(key.T, source_ref[...]))
        terms = (jnp.concatenate(terms, axis=0) * weight_scale).astype(BF16)
        terms = shuffled(terms, z_count, y_count, own)
        for y in range(y_count):
            out_ref[y] = terms[y * z_count * own : (y + 1) * z_count * own, :]

    return pl.pallas_call(
        kernel,
        in_specs=[in_vmem()] * 2,
        out_specs=in_vmem(),
        out_shape=jax.ShapeDtypeStruct((y_count, z_count * own, source.shape[1]), BF16),
        compiler_params=pltpu.CompilerParams(vmem_limit_bytes=SMALL_VMEM_LIMIT),
        name="key_products",
    )(halves, source)


def joined(keys, keep, arrived):
    y_count, rows, width = keys.shape
    z_count, quarter, dim = keep.shape
    own = rows // z_count
    wide = width // dim

    def kernel(keys_ref, keep_ref, arrived_ref, out_ref):
        total = sum(keys_ref[y].astype(F32) for y in range(y_count)).astype(BF16)
        blocks = [total[:, b * dim : (b + 1) * dim] for b in range(wide)]
        blocks = shuffled(jnp.concatenate(blocks, axis=0), wide, z_count, own)
        dq = keep_ref[...].astype(F32) + arrived_ref[...].astype(F32)
        out_ref[:, :quarter, :] = dq.astype(BF16)
        for z in range(z_count):
            out_ref[z, quarter:, :] = blocks[z * wide * own : (z + 1) * wide * own, :]

    return pl.pallas_call(
        kernel,
        in_specs=[in_vmem()] * 3,
        out_specs=in_vmem(),
        out_shape=jax.ShapeDtypeStruct((z_count, quarter + wide * own, dim), BF16),
        compiler_params=pltpu.CompilerParams(vmem_limit_bytes=SMALL_VMEM_LIMIT),
        name="joined",
    )(keys, keep, arrived)


def split_sums(blocks, rows, width):
    z_count, height, dim = blocks.shape
    quarter = rows // 4
    wide = width // dim
    own = (height - quarter) // wide

    def kernel(blocks_ref, dq_ref, keys_ref):
        for turn in range(4):
            first = turn % 2 * 2 + turn // 2
            dq_ref[first * quarter : (first + 1) * quarter, :] = sum(
                blocks_ref[z, :quarter, :].astype(F32) for z in range(turn, z_count, 4)
            )
        keys = sum(blocks_ref[z, quarter:, :].astype(F32) for z in range(z_count))
        for b in range(wide):
            keys_ref[:, b * dim : (b + 1) * dim] = keys[b * own : (b + 1) * own, :]

    return pl.pallas_call(
        kernel,
        in_specs=[in_vmem()],
        out_specs=[in_vmem()] * 2,
        out_shape=[
            jax.ShapeDtypeStruct((rows, dim), F32),
            jax.ShapeDtypeStruct((own, width), F32),
        ],
        compiler_params=pltpu.CompilerParams(vmem_limit_bytes=SMALL_VMEM_LIMIT),
        name="split_sums",
    )(blocks)


def shards(
    queries, attn_out, out_grad, row_lse, source, saved_keys, saved_values, key_weight, value_weight
):
    src = source.shape[0]
    tp_count = SPLIT[2] * SPLIT[3] * SPLIT[4]
    sp_count = SPLIT[0] * SPLIT[1]
    weight_scale = 1.0 / math.sqrt(src * sp_count)
    main, last, keyvals = pack_rows(
        queries, attn_out, out_grad, row_lse, saved_keys, saved_values
    )
    keyvals = exchanged(keyvals, "y")
    main = lax.all_gather(main, "z", axis=0, tiled=False)
    last = exchanged(last, "z")
    before = attention_backward(main, keyvals)
    me = jnp.bitwise_and(lax.axis_index("z"), 1).reshape(1)
    dq_send, dq_keep, dkv = attention_backward(main, keyvals, last, before, me)

    dkv = exchanged(dkv, TEAM)
    halves = added_up(dkv, tp_count)
    halves = exchanged(halves, TP)
    dq_keep, dq_arrived = rows_by_turns(dq_send, dq_keep)
    key_terms = key_products(halves, source, weight_scale)
    key_terms = exchanged(key_terms, "y")
    blocks = joined(key_terms, dq_keep, dq_arrived)
    blocks = exchanged(blocks, "z")
    query_grad, key_grad = split_sums(blocks, queries.shape[0], source.shape[1])
    halves = halves.reshape(2, tp_count // 2, 2, -1, HEAD_DIM)
    key_half, value_half = (halves[:, :, i].reshape(2, src, HEAD_DIM) for i in range(2))
    weights = jnp.concatenate([key_weight, value_weight], axis=1)
    source_grad = lax.dot_general(
        jnp.concatenate([key_half[0], key_half[1], value_half[0], value_half[1]], axis=1),
        weights,
        (((1,), (1,)), ((), ())),
        preferred_element_type=F32,
    )
    return (query_grad, source_grad, key_grad)


def solution(mesh):
    split = Mesh(mesh.devices.reshape(SPLIT), ("z", "y", "g", "h", "c"))
    return jax.shard_map(
        shards,
        mesh=split,
        in_specs=(
            P(SP, TP),
            P(SP, TP),
            P(SP, TP),
            P(SP, TP),
            P(SP, TP),
            P(SP, None),
            P(SP, None),
            P(TP, None),
            P(TP, None),
        ),
        out_specs=(P(SP, TP), P(SP, TP), P(SP, TP)),
        check_vma=False,
    )
```

```python
import math

import jax
import jax.numpy as jnp
from jax import lax
from jax.experimental import pallas as pl
from jax.experimental.pallas import tpu as pltpu
from jax.sharding import Mesh
from jax.sharding import PartitionSpec as P


HEAD_DIM = 128
SP = ("z", "y")
TP = ("g", "h", "c")
TEAM = ("y", "h", "c")
SPLIT = (16, 4, 2, 2, 2)
F32 = jnp.float32
BF16 = jnp.bfloat16
FIRST = 96
STAT_ROWS = 16
FIRST_VMEM_LIMIT = 18 * 2**20
LAST_VMEM_LIMIT = 20 * 2**20
SMALL_VMEM_LIMIT = 8 * 2**20


def in_vmem():
    return pl.BlockSpec(memory_space=pltpu.VMEM)


def pieces(value):
    high = value.astype(BF16)
    rest = value - high.astype(F32)
    middle = rest.astype(BF16)
    low = (rest - middle.astype(F32)).astype(BF16)
    return [high, middle, low]


def pack_rows(queries, attn_out, out_grad, row_lse, saved_keys, saved_values):
    rows, width = queries.shape
    src = saved_keys.shape[0]
    z_count, y_count = (SPLIT[0], SPLIT[1])

    def kernel(head_ref, q_ref, o_ref, do_ref, lse_ref, k_ref, v_ref, main_ref, last_ref, kv_ref):
        second = head_ref[0] > 0
        main_ref[:rows, :] = q_ref[...]
        main_ref[rows : rows + FIRST, :] = do_ref[:FIRST, :]
        product = do_ref[...].astype(F32) * o_ref[...].astype(F32)
        delta = jnp.sum(product.T, axis=0, keepdims=True)
        stats = pieces(lse_ref[...] * math.sqrt(HEAD_DIM)) + pieces(delta)
        line = lax.broadcasted_iota(jnp.int32, (STAT_ROWS, rows), 0)
        block = jnp.zeros((STAT_ROWS, rows), F32)
        for i, s in enumerate(stats):
            block = jnp.where(line == i, s.astype(F32), block)
        main_ref[rows + FIRST :, :] = block.astype(BF16)
        last = do_ref[FIRST:, :]
        for z in range(z_count):
            last_ref[z] = last
        k = jnp.where(second, k_ref[:, HEAD_DIM:], k_ref[:, :HEAD_DIM])
        v = jnp.where(second, v_ref[:, HEAD_DIM:], v_ref[:, :HEAD_DIM])
        for y in range(y_count):
            kv_ref[y, :src, :] = k
            kv_ref[y, src:, :] = v

    return pl.pallas_call(
        kernel,
        in_specs=[pl.BlockSpec(memory_space=pltpu.SMEM)] + [in_vmem()] * 6,
        out_specs=[in_vmem()] * 3,
        out_shape=[
            jax.ShapeDtypeStruct((rows + FIRST + STAT_ROWS, width), BF16),
            jax.ShapeDtypeStruct((z_count, rows - FIRST, width), BF16),
            jax.ShapeDtypeStruct((y_count, 2 * src, HEAD_DIM), BF16),
        ],
        name="pack_rows",
    )(
        lax.axis_index("g").reshape(1),
        queries,
        attn_out,
        out_grad,
        row_lse.reshape(1, rows),
        saved_keys,
        saved_values,
    )


def dot(left, right):
    return jnp.dot(left, right, preferred_element_type=F32)


def attention_backward(main, keyvals, last=None, before=None, me=None):
    z_count, main_rows, dim = main.shape
    y_count, src = (keyvals.shape[0], keyvals.shape[1] // 2)
    rows = main_rows - FIRST - STAT_ROWS
    low, high = (0, FIRST) if last is None else (FIRST, rows)
    each = high - low
    sources, targets = (y_count * src, z_count * each)
    scale = 1.0 / math.sqrt(HEAD_DIM)
    exp_scale = math.log2(math.e) * scale
    src_tile, tgt_tile = (512, 512)
    team = y_count * SPLIT[3] * SPLIT[4]
    piece = sources // team

    def prepare(main_ref, kv_ref, last_ref, k_wide, v_wide, k_turned, q_turned, do_turned, q_rows, do_rows):
        lane = lax.broadcasted_iota(jnp.int32, (src, dim), 1)
        lse_lanes = jnp.where(lane < 3, -1.0, 0.0).astype(BF16)
        delta_lanes = jnp.where((lane >= 3) & (lane < 6), -1.0, 0.0).astype(BF16)
        for y in range(y_count):
            at = slice(y * src, (y + 1) * src)
            k = kv_ref[y, :src, :]
            k_wide[at, :dim] = k
            k_wide[at, dim:] = lse_lanes
            v_wide[at, :dim] = kv_ref[y, src:, :]
            v_wide[at, dim:] = delta_lanes
            k_turned[:, at] = k.T
        blank = jnp.zeros((dim - STAT_ROWS, dim), BF16)
        for z in range(z_count):
            at = slice(z * each, (z + 1) * each)
            q_rows[at, :dim] = main_ref[z, low:high, :]
            stats = jnp.concatenate([main_ref[z, rows + FIRST :, :], blank], axis=0)
            q_rows[at, dim:] = stats.T[low:high, :]
            do_rows[at, :] = main_ref[z, rows : rows + FIRST, :] if last_ref is None else last_ref[z]
        for b in range(0, targets, dim):
            at = slice(b, b + dim)
            q_turned[:dim, at] = q_rows[at, :dim].T
            stats = q_rows[at, dim:].T
            q_turned[dim:, at] = stats
            do_turned[:dim, at] = do_rows[at, :].T
            do_turned[dim:, at] = stats

    def work(k_wide, v_wide, k_turned, q_turned, do_turned, q_rows, do_rows, dk_acc, dv_acc, dq_acc):
        def step(i, carry):
            s = pl.ds(pl.multiple_of(i * src_tile, src_tile), src_tile)
            for t0 in range(0, targets, tgt_tile):
                t = slice(t0, t0 + tgt_tile)
                scores = dot(k_wide[s, :], q_turned[:, t])
                dprobs = dot(v_wide[s, :], do_turned[:, t])
                probs = jnp.exp2(scores * exp_scale)
                dscores = (probs * dprobs).astype(BF16)
                dv_acc[s, :] += dot(probs.astype(BF16), do_rows[t, :])
                dk_acc[s, :] += dot(dscores, q_rows[t, :dim])
                dq_acc[:, t] += dot(k_turned[:, s], dscores)
            return carry

        dk_acc[...] = jnp.zeros_like(dk_acc)
        dv_acc[...] = jnp.zeros_like(dv_acc)
        dq_acc[...] = jnp.zeros_like(dq_acc)
        lax.fori_loop(0, sources // src_tile, step, 0)

    def first_kernel(main_ref, kv_ref, out_ref, *scratch):
        dk_acc, dv_acc, dq_acc = scratch[-3:]
        prepare(main_ref, kv_ref, None, *scratch[:-3])
        work(*scratch)
        out_ref[:sources, :] = (dk_acc[...] * scale).astype(BF16)
        out_ref[sources : 2 * sources, :] = dv_acc[...].astype(BF16)
        for b in range(0, targets, dim):
            turned = (dq_acc[:, b : b + dim] * scale).T.astype(BF16)
            out_ref[2 * sources + b : 2 * sources + b + dim, :] = turned

    def last_kernel(
        me_ref, main_ref, kv_ref, last_ref, before_ref, send_ref, keep_ref, dkv_ref, *scratch
    ):
        dk_acc, dv_acc, dq_acc, dq_rows = scratch[-4:]
        prepare(main_ref, kv_ref, last_ref, *scratch[:-4])
        work(*scratch[:-1])
        for i in range(team):
            at = slice(i * piece, (i + 1) * piece)
            dk_before = before_ref[at, :].astype(F32)
            dv_before = before_ref[sources + i * piece : sources + (i + 1) * piece, :].astype(F32)
            dkv_ref[i, :piece, :] = (dk_acc[at, :] * scale + dk_before).astype(BF16)
            dkv_ref[i, piece:, :] = (dv_acc[at, :] + dv_before).astype(BF16)
        for z in range(z_count // 4):
            at = slice(z * 4 * each, (z + 1) * 4 * each)
            turned = (dq_acc[:, at] * scale).T.astype(BF16)
            for i in range(4):
                dq_rows[z * 4 + i] = turned[i * each : (i + 1) * each, :]
        half_rows = rows // 2
        for odd, (low_ref, high_ref) in enumerate(((keep_ref, send_ref), (send_ref, keep_ref))):

            @pl.when(me_ref[0] == odd)
            def _(low_ref=low_ref, high_ref=high_ref):
                for z in range(z_count):
                    at = 2 * sources + z * FIRST
                    low_ref[z] = before_ref[at : at + half_rows, :]
                    high_ref[z, : FIRST - half_rows, :] = before_ref[at + half_rows : at + FIRST, :]
                high_ref[:, FIRST - half_rows :, :] = dq_rows[...]

    dkv = pltpu.MemorySpace.HBM((team, 2 * piece, dim), BF16)
    scratch = [
        pltpu.VMEM((sources, 2 * dim), BF16),
        pltpu.VMEM((sources, 2 * dim), BF16),
        pltpu.VMEM((dim, sources), BF16),
        pltpu.VMEM((2 * dim, targets), BF16),
        pltpu.VMEM((2 * dim, targets), BF16),
        pltpu.VMEM((targets, 2 * dim), BF16),
        pltpu.VMEM((targets, dim), BF16),
        pltpu.VMEM((sources, dim), F32),
        pltpu.VMEM((sources, dim), F32),
        pltpu.VMEM((dim, targets), F32),
    ]
    if last is None:
        return pl.pallas_call(
            first_kernel,
            in_specs=[in_vmem()] * 2,
            out_specs=in_vmem(),
            out_shape=jax.ShapeDtypeStruct((2 * sources + targets, dim), BF16),
            scratch_shapes=scratch,
            compiler_params=pltpu.CompilerParams(vmem_limit_bytes=FIRST_VMEM_LIMIT),
            name="attention_first",
        )(main, keyvals)
    half = pltpu.MemorySpace.HBM((z_count, rows // 2, dim), BF16)
    return pl.pallas_call(
        last_kernel,
        in_specs=[pl.BlockSpec(memory_space=pltpu.SMEM)] + [in_vmem()] * 4,
        out_specs=[in_vmem()] * 3,
        out_shape=[half, half, dkv],
        scratch_shapes=scratch + [pltpu.VMEM((z_count, each, dim), BF16)],
        compiler_params=pltpu.CompilerParams(vmem_limit_bytes=LAST_VMEM_LIMIT),
        name="attention_last",
    )(me, main, keyvals, last, before)


def added_up(arrived, copies):
    total = jnp.sum(arrived.astype(F32), axis=0).astype(BF16)
    return jnp.broadcast_to(total[None], (copies, *total.shape))


def exchanged(value, axes):
    return lax.all_to_all(value, axes, 0, 0, tiled=True)


def swapped(value, axis, distance):
    pairs = [(i, i ^ distance) for i in range(lax.axis_size(axis))]
    return lax.ppermute(value, axis, pairs)


def rows_by_turns(send, keep):
    arrived = swapped(send, "z", 1)
    for distance in (1, 2):
        count = keep.shape[1] // 2
        mine = jnp.bitwise_and(lax.axis_index("z"), 2 * distance)

        def part(first):
            a, b = (jnp.where(first, v[:, :count], v[:, count:]) for v in (keep, arrived))
            return (a.astype(F32) + b.astype(F32)).astype(BF16)

        send = part(mine > 0)
        keep, arrived = lax.optimization_barrier((keep, arrived))
        keep = part(mine == 0)
        arrived = swapped(send, "z", 2 * distance)
    return keep, arrived


def shuffled(value, outer, middle, inner):
    rows = outer * middle * inner
    new = lax.broadcasted_iota(jnp.int32, (rows, rows), 0)
    old = lax.broadcasted_iota(jnp.int32, (rows, rows), 1)
    m, o, i = (new // (outer * inner), new // inner % outer, new % inner)
    take = old == (o * middle + m) * inner + i
    return dot(jnp.where(take, 1.0, 0.0).astype(BF16), value).astype(BF16)


def key_products(halves, source, weight_scale):
    parts, rows, dim = halves.shape
    z_count, y_count = (SPLIT[0], SPLIT[1])
    own = 2 * dim // (z_count * y_count)

    def kernel(halves_ref, source_ref, out_ref):
        terms = []
        for g in range(2):
            key = jnp.concatenate(
                [halves_ref[g * parts // 2 + p, : rows // 2, :] for p in range(parts // 2)], axis=0
            )
            terms.append(dot(key.T, source_ref[...]))
        terms = (jnp.concatenate(terms, axis=0) * weight_scale).astype(BF16)
        terms = shuffled(terms, z_count, y_count, own)
        for y in range(y_count):
            out_ref[y] = terms[y * z_count * own : (y + 1) * z_count * own, :]

    return pl.pallas_call(
        kernel,
        in_specs=[in_vmem()] * 2,
        out_specs=in_vmem(),
        out_shape=jax.ShapeDtypeStruct((y_count, z_count * own, source.shape[1]), BF16),
        compiler_params=pltpu.CompilerParams(vmem_limit_bytes=SMALL_VMEM_LIMIT),
        name="key_products",
    )(halves, source)


def joined(keys, keep, arrived):
    y_count, rows, width = keys.shape
    z_count, share, dim = keep.shape
    own = rows // z_count
    wide = width // dim

    def kernel(keys_ref, keep_ref, arrived_ref, out_ref):
        total = sum(keys_ref[y].astype(F32) for y in range(y_count)).astype(BF16)
        blocks = [total[:, b * dim : (b + 1) * dim] for b in range(wide)]
        blocks = shuffled(jnp.concatenate(blocks, axis=0), wide, z_count, own)
        dq = keep_ref[...].astype(F32) + arrived_ref[...].astype(F32)
        out_ref[:, :share, :] = dq.astype(BF16)
        for z in range(z_count):
            out_ref[z, share:, :] = blocks[z * wide * own : (z + 1) * wide * own, :]

    return pl.pallas_call(
        kernel,
        in_specs=[in_vmem()] * 3,
        out_specs=in_vmem(),
        out_shape=jax.ShapeDtypeStruct((z_count, share + wide * own, dim), BF16),
        compiler_params=pltpu.CompilerParams(vmem_limit_bytes=SMALL_VMEM_LIMIT),
        name="joined",
    )(keys, keep, arrived)


def split_sums(blocks, rows, width):
    z_count, height, dim = blocks.shape
    share = rows // 8
    wide = width // dim
    own = (height - share) // wide

    def kernel(blocks_ref, dq_ref, keys_ref):
        for turn in range(8):
            first = turn % 2 * 4 + turn // 2 % 2 * 2 + turn // 4
            dq_ref[first * share : (first + 1) * share, :] = sum(
                blocks_ref[z, :share, :].astype(F32) for z in range(turn, z_count, 8)
            )
        keys = sum(blocks_ref[z, share:, :].astype(F32) for z in range(z_count))
        for b in range(wide):
            keys_ref[:, b * dim : (b + 1) * dim] = keys[b * own : (b + 1) * own, :]

    return pl.pallas_call(
        kernel,
        in_specs=[in_vmem()],
        out_specs=[in_vmem()] * 2,
        out_shape=[
            jax.ShapeDtypeStruct((rows, dim), F32),
            jax.ShapeDtypeStruct((own, width), F32),
        ],
        compiler_params=pltpu.CompilerParams(vmem_limit_bytes=SMALL_VMEM_LIMIT),
        name="split_sums",
    )(blocks)


def shards(
    queries, attn_out, out_grad, row_lse, source, saved_keys, saved_values, key_weight, value_weight
):
    src = source.shape[0]
    tp_count = SPLIT[2] * SPLIT[3] * SPLIT[4]
    sp_count = SPLIT[0] * SPLIT[1]
    weight_scale = 1.0 / math.sqrt(src * sp_count)
    main, last, keyvals = pack_rows(
        queries, attn_out, out_grad, row_lse, saved_keys, saved_values
    )
    keyvals = exchanged(keyvals, "y")
    main = lax.all_gather(main, "z", axis=0, tiled=False)
    last = exchanged(last, "z")
    before = attention_backward(main, keyvals)
    me = jnp.bitwise_and(lax.axis_index("z"), 1).reshape(1)
    dq_send, dq_keep, dkv = attention_backward(main, keyvals, last, before, me)

    dkv = exchanged(dkv, TEAM)
    halves = added_up(dkv, tp_count)
    halves = exchanged(halves, TP)
    dq_keep, dq_arrived = rows_by_turns(dq_send, dq_keep)
    key_terms = key_products(halves, source, weight_scale)
    key_terms = exchanged(key_terms, "y")
    blocks = joined(key_terms, dq_keep, dq_arrived)
    blocks = exchanged(blocks, "z")
    query_grad, key_grad = split_sums(blocks, queries.shape[0], source.shape[1])
    halves = halves.reshape(2, tp_count // 2, 2, -1, HEAD_DIM)
    key_half, value_half = (halves[:, :, i].reshape(2, src, HEAD_DIM) for i in range(2))
    weights = jnp.concatenate([key_weight, value_weight], axis=1)
    source_grad = lax.dot_general(
        jnp.concatenate([key_half[0], key_half[1], value_half[0], value_half[1]], axis=1),
        weights,
        (((1,), (1,)), ((), ())),
        preferred_element_type=F32,
    )
    return (query_grad, source_grad, key_grad)


def solution(mesh):
    split = Mesh(mesh.devices.reshape(SPLIT), ("z", "y", "g", "h", "c"))
    return jax.shard_map(
        shards,
        mesh=split,
        in_specs=(
            P(SP, TP),
            P(SP, TP),
            P(SP, TP),
            P(SP, TP),
            P(SP, TP),
            P(SP, None),
            P(SP, None),
            P(TP, None),
            P(TP, None),
        ),
        out_specs=(P(SP, TP), P(SP, TP), P(SP, TP)),
        check_vma=False,
    )
```

```python
import math

import jax
import jax.numpy as jnp
from jax import lax
from jax.experimental import pallas as pl
from jax.experimental.pallas import tpu as pltpu
from jax.sharding import Mesh
from jax.sharding import PartitionSpec as P


HEAD_DIM = 128
SP = ("z", "y")
TP = ("g", "h", "c")
TEAM = ("y", "h", "c")
SPLIT = (16, 4, 2, 2, 2)
F32 = jnp.float32
BF16 = jnp.bfloat16
FIRST = 96
STAT_ROWS = 16
FIRST_VMEM_LIMIT = 24 * 2**20
LAST_VMEM_LIMIT = 24 * 2**20
SMALL_VMEM_LIMIT = 8 * 2**20


def in_vmem():
    return pl.BlockSpec(memory_space=pltpu.VMEM)


def pieces(value):
    high = value.astype(BF16)
    rest = value - high.astype(F32)
    middle = rest.astype(BF16)
    low = (rest - middle.astype(F32)).astype(BF16)
    return [high, middle, low]


def pack_rows(queries, attn_out, out_grad, row_lse, saved_keys, saved_values):
    rows, width = queries.shape
    src = saved_keys.shape[0]
    z_count, y_count = (SPLIT[0], SPLIT[1])

    def kernel(head_ref, q_ref, o_ref, do_ref, lse_ref, k_ref, v_ref, main_ref, last_ref, kv_ref):
        second = head_ref[0] > 0
        main_ref[:rows, :] = q_ref[...]
        main_ref[rows : rows + FIRST, :] = do_ref[:FIRST, :]
        product = do_ref[...].astype(F32) * o_ref[...].astype(F32)
        delta = jnp.sum(product.T, axis=0, keepdims=True)
        stats = pieces(lse_ref[...] * math.sqrt(HEAD_DIM)) + pieces(delta)
        line = lax.broadcasted_iota(jnp.int32, (STAT_ROWS, rows), 0)
        block = jnp.zeros((STAT_ROWS, rows), F32)
        for i, s in enumerate(stats):
            block = jnp.where(line == i, s.astype(F32), block)
        main_ref[rows + FIRST :, :] = block.astype(BF16)
        last = do_ref[FIRST:, :]
        for z in range(z_count):
            last_ref[z] = last
        k = jnp.where(second, k_ref[:, HEAD_DIM:], k_ref[:, :HEAD_DIM])
        v = jnp.where(second, v_ref[:, HEAD_DIM:], v_ref[:, :HEAD_DIM])
        for y in range(y_count):
            kv_ref[y, :src, :] = k
            kv_ref[y, src:, :] = v

    return pl.pallas_call(
        kernel,
        in_specs=[pl.BlockSpec(memory_space=pltpu.SMEM)] + [in_vmem()] * 6,
        out_specs=[in_vmem()] * 3,
        out_shape=[
            jax.ShapeDtypeStruct((rows + FIRST + STAT_ROWS, width), BF16),
            jax.ShapeDtypeStruct((z_count, rows - FIRST, width), BF16),
            jax.ShapeDtypeStruct((y_count, 2 * src, HEAD_DIM), BF16),
        ],
        name="pack_rows",
    )(
        lax.axis_index("g").reshape(1),
        queries,
        attn_out,
        out_grad,
        row_lse.reshape(1, rows),
        saved_keys,
        saved_values,
    )


def dot(left, right):
    return jnp.dot(left, right, preferred_element_type=F32)


def attention_backward(main, keyvals, last=None, before=None, me=None):
    z_count, main_rows, dim = main.shape
    y_count, src = (keyvals.shape[0], keyvals.shape[1] // 2)
    rows = main_rows - FIRST - STAT_ROWS
    low, high = (0, FIRST) if last is None else (FIRST, rows)
    each = high - low
    sources, targets = (y_count * src, z_count * each)
    scale = 1.0 / math.sqrt(HEAD_DIM)
    exp_scale = math.log2(math.e) * scale
    src_tile, tgt_tile = (1024, 512)
    team = y_count * SPLIT[3] * SPLIT[4]
    piece = sources // team

    def prepare(main_ref, kv_ref, last_ref, k_wide, v_wide, k_turned, q_turned, do_turned, q_rows, do_rows):
        lane = lax.broadcasted_iota(jnp.int32, (src, dim), 1)
        lse_lanes = jnp.where(lane < 3, -1.0, 0.0).astype(BF16)
        delta_lanes = jnp.where((lane >= 3) & (lane < 6), -1.0, 0.0).astype(BF16)
        for y in range(y_count):
            at = slice(y * src, (y + 1) * src)
            k = kv_ref[y, :src, :]
            k_wide[at, :dim] = k
            k_wide[at, dim:] = lse_lanes
            v_wide[at, :dim] = kv_ref[y, src:, :]
            v_wide[at, dim:] = delta_lanes
            k_turned[:, at] = k.T
        blank = jnp.zeros((dim - STAT_ROWS, dim), BF16)
        for z in range(z_count):
            at = slice(z * each, (z + 1) * each)
            q_rows[at, :dim] = main_ref[z, low:high, :]
            stats = jnp.concatenate([main_ref[z, rows + FIRST :, :], blank], axis=0)
            q_rows[at, dim:] = stats.T[low:high, :]
            do_rows[at, :] = main_ref[z, rows : rows + FIRST, :] if last_ref is None else last_ref[z]
        for b in range(0, targets, dim):
            at = slice(b, b + dim)
            q_turned[:dim, at] = q_rows[at, :dim].T
            stats = q_rows[at, dim:].T
            q_turned[dim:, at] = stats
            do_turned[:dim, at] = do_rows[at, :].T
            do_turned[dim:, at] = stats

    def work(k_wide, v_wide, k_turned, q_turned, do_turned, q_rows, do_rows, dk_acc, dv_acc, dq_acc):
        def step(i, carry):
            s = pl.ds(pl.multiple_of(i * src_tile, src_tile), src_tile)
            for t0 in range(0, targets, tgt_tile):
                t = slice(t0, t0 + tgt_tile)
                scores = dot(k_wide[s, :], q_turned[:, t])
                dprobs = dot(v_wide[s, :], do_turned[:, t])
                probs = jnp.exp2(scores * exp_scale)
                dscores = (probs * dprobs).astype(BF16)
                dv_acc[s, :] += dot(probs.astype(BF16), do_rows[t, :])
                dk_acc[s, :] += dot(dscores, q_rows[t, :dim])
                dq_acc[:, t] += dot(k_turned[:, s], dscores)
            return carry

        dk_acc[...] = jnp.zeros_like(dk_acc)
        dv_acc[...] = jnp.zeros_like(dv_acc)
        dq_acc[...] = jnp.zeros_like(dq_acc)
        lax.fori_loop(0, sources // src_tile, step, 0)

    def first_kernel(main_ref, kv_ref, out_ref, *scratch):
        dk_acc, dv_acc, dq_acc = scratch[-3:]
        prepare(main_ref, kv_ref, None, *scratch[:-3])
        work(*scratch)
        out_ref[:sources, :] = (dk_acc[...] * scale).astype(BF16)
        out_ref[sources : 2 * sources, :] = dv_acc[...].astype(BF16)
        for b in range(0, targets, dim):
            turned = (dq_acc[:, b : b + dim] * scale).T.astype(BF16)
            out_ref[2 * sources + b : 2 * sources + b + dim, :] = turned

    def last_kernel(
        me_ref, main_ref, kv_ref, last_ref, before_ref, send_ref, keep_ref, dkv_ref, *scratch
    ):
        dk_acc, dv_acc, dq_acc, dq_rows = scratch[-4:]
        prepare(main_ref, kv_ref, last_ref, *scratch[:-4])
        work(*scratch[:-1])
        for i in range(team):
            at = slice(i * piece, (i + 1) * piece)
            dk_before = before_ref[at, :].astype(F32)
            dv_before = before_ref[sources + i * piece : sources + (i + 1) * piece, :].astype(F32)
            dkv_ref[i, :piece, :] = (dk_acc[at, :] * scale + dk_before).astype(BF16)
            dkv_ref[i, piece:, :] = (dv_acc[at, :] + dv_before).astype(BF16)
        for z in range(z_count // 4):
            at = slice(z * 4 * each, (z + 1) * 4 * each)
            turned = (dq_acc[:, at] * scale).T.astype(BF16)
            for i in range(4):
                dq_rows[z * 4 + i] = turned[i * each : (i + 1) * each, :]
        half_rows = rows // 2
        for odd, (low_ref, high_ref) in enumerate(((keep_ref, send_ref), (send_ref, keep_ref))):

            @pl.when(me_ref[0] == odd)
            def _(low_ref=low_ref, high_ref=high_ref):
                for z in range(z_count):
                    at = 2 * sources + z * FIRST
                    low_ref[z] = before_ref[at : at + half_rows, :]
                    high_ref[z, : FIRST - half_rows, :] = before_ref[at + half_rows : at + FIRST, :]
                high_ref[:, FIRST - half_rows :, :] = dq_rows[...]

    dkv = pltpu.MemorySpace.HBM((team, 2 * piece, dim), BF16)
    scratch = [
        pltpu.VMEM((sources, 2 * dim), BF16),
        pltpu.VMEM((sources, 2 * dim), BF16),
        pltpu.VMEM((dim, sources), BF16),
        pltpu.VMEM((2 * dim, targets), BF16),
        pltpu.VMEM((2 * dim, targets), BF16),
        pltpu.VMEM((targets, 2 * dim), BF16),
        pltpu.VMEM((targets, dim), BF16),
        pltpu.VMEM((sources, dim), F32),
        pltpu.VMEM((sources, dim), F32),
        pltpu.VMEM((dim, targets), F32),
    ]
    if last is None:
        return pl.pallas_call(
            first_kernel,
            in_specs=[in_vmem()] * 2,
            out_specs=in_vmem(),
            out_shape=jax.ShapeDtypeStruct((2 * sources + targets, dim), BF16),
            scratch_shapes=scratch,
            compiler_params=pltpu.CompilerParams(vmem_limit_bytes=FIRST_VMEM_LIMIT),
            name="attention_first",
        )(main, keyvals)
    half = pltpu.MemorySpace.HBM((z_count, rows // 2, dim), BF16)
    return pl.pallas_call(
        last_kernel,
        in_specs=[pl.BlockSpec(memory_space=pltpu.SMEM)] + [in_vmem()] * 4,
        out_specs=[in_vmem()] * 3,
        out_shape=[half, half, dkv],
        scratch_shapes=scratch + [pltpu.VMEM((z_count, each, dim), BF16)],
        compiler_params=pltpu.CompilerParams(vmem_limit_bytes=LAST_VMEM_LIMIT),
        name="attention_last",
    )(me, main, keyvals, last, before)


def added_up(arrived, copies):
    count, rows, width = arrived.shape

    def kernel(arrived_ref, out_ref):
        total = sum(arrived_ref[i].astype(F32) for i in range(count)).astype(BF16)
        for i in range(copies):
            out_ref[i] = total

    return pl.pallas_call(
        kernel,
        in_specs=[in_vmem()],
        out_specs=in_vmem(),
        out_shape=pltpu.MemorySpace.HBM((copies, rows, width), BF16),
        compiler_params=pltpu.CompilerParams(vmem_limit_bytes=SMALL_VMEM_LIMIT),
        name="added_up",
    )(arrived)


def exchanged(value, axes):
    return lax.all_to_all(value, axes, 0, 0, tiled=True)


def swapped(value, axis, distance):
    pairs = [(i, i ^ distance) for i in range(lax.axis_size(axis))]
    return lax.ppermute(value, axis, pairs)


def rows_by_turns(send, keep):
    arrived = swapped(send, "z", 1)
    for distance in (1, 2):
        count = keep.shape[1] // 2
        mine = jnp.bitwise_and(lax.axis_index("z"), 2 * distance)

        def part(first):
            a, b = (jnp.where(first, v[:, :count], v[:, count:]) for v in (keep, arrived))
            return (a.astype(F32) + b.astype(F32)).astype(BF16)

        send = part(mine > 0)
        keep, arrived = lax.optimization_barrier((keep, arrived))
        keep = part(mine == 0)
        arrived = swapped(send, "z", 2 * distance)
    return keep, arrived


def shuffled(value, outer, middle, inner):
    rows = outer * middle * inner
    new = lax.broadcasted_iota(jnp.int32, (rows, rows), 0)
    old = lax.broadcasted_iota(jnp.int32, (rows, rows), 1)
    m, o, i = (new // (outer * inner), new // inner % outer, new % inner)
    take = old == (o * middle + m) * inner + i
    return dot(jnp.where(take, 1.0, 0.0).astype(BF16), value).astype(BF16)


def key_products(halves, source, weight_scale):
    parts, rows, dim = halves.shape
    z_count, y_count = (SPLIT[0], SPLIT[1])
    own = 2 * dim // (z_count * y_count)

    def kernel(halves_ref, source_ref, out_ref):
        terms = []
        for g in range(2):
            key = jnp.concatenate(
                [halves_ref[g * parts // 2 + p, : rows // 2, :] for p in range(parts // 2)], axis=0
            )
            terms.append(dot(key.T, source_ref[...]))
        terms = (jnp.concatenate(terms, axis=0) * weight_scale).astype(BF16)
        terms = shuffled(terms, z_count, y_count, own)
        for y in range(y_count):
            out_ref[y] = terms[y * z_count * own : (y + 1) * z_count * own, :]

    return pl.pallas_call(
        kernel,
        in_specs=[in_vmem()] * 2,
        out_specs=in_vmem(),
        out_shape=jax.ShapeDtypeStruct((y_count, z_count * own, source.shape[1]), BF16),
        compiler_params=pltpu.CompilerParams(vmem_limit_bytes=SMALL_VMEM_LIMIT),
        name="key_products",
    )(halves, source)


def joined(keys, keep, arrived):
    y_count, rows, width = keys.shape
    z_count, share, dim = keep.shape
    own = rows // z_count
    wide = width // dim

    def kernel(keys_ref, keep_ref, arrived_ref, out_ref):
        total = sum(keys_ref[y].astype(F32) for y in range(y_count)).astype(BF16)
        blocks = [total[:, b * dim : (b + 1) * dim] for b in range(wide)]
        blocks = shuffled(jnp.concatenate(blocks, axis=0), wide, z_count, own)
        dq = keep_ref[...].astype(F32) + arrived_ref[...].astype(F32)
        out_ref[:, :share, :] = dq.astype(BF16)
        for z in range(z_count):
            out_ref[z, share:, :] = blocks[z * wide * own : (z + 1) * wide * own, :]

    return pl.pallas_call(
        kernel,
        in_specs=[in_vmem()] * 3,
        out_specs=in_vmem(),
        out_shape=jax.ShapeDtypeStruct((z_count, share + wide * own, dim), BF16),
        compiler_params=pltpu.CompilerParams(vmem_limit_bytes=SMALL_VMEM_LIMIT),
        name="joined",
    )(keys, keep, arrived)


def split_sums(blocks, rows, width):
    z_count, height, dim = blocks.shape
    share = rows // 8
    wide = width // dim
    own = (height - share) // wide

    def kernel(blocks_ref, dq_ref, keys_ref):
        for turn in range(8):
            first = turn % 2 * 4 + turn // 2 % 2 * 2 + turn // 4
            dq_ref[first * share : (first + 1) * share, :] = sum(
                blocks_ref[z, :share, :].astype(F32) for z in range(turn, z_count, 8)
            )
        keys = sum(blocks_ref[z, share:, :].astype(F32) for z in range(z_count))
        for b in range(wide):
            keys_ref[:, b * dim : (b + 1) * dim] = keys[b * own : (b + 1) * own, :]

    return pl.pallas_call(
        kernel,
        in_specs=[in_vmem()],
        out_specs=[in_vmem()] * 2,
        out_shape=[
            jax.ShapeDtypeStruct((rows, dim), F32),
            jax.ShapeDtypeStruct((own, width), F32),
        ],
        compiler_params=pltpu.CompilerParams(vmem_limit_bytes=SMALL_VMEM_LIMIT),
        name="split_sums",
    )(blocks)


def shards(
    queries, attn_out, out_grad, row_lse, source, saved_keys, saved_values, key_weight, value_weight
):
    src = source.shape[0]
    tp_count = SPLIT[2] * SPLIT[3] * SPLIT[4]
    sp_count = SPLIT[0] * SPLIT[1]
    weight_scale = 1.0 / math.sqrt(src * sp_count)
    main, last, keyvals = pack_rows(
        queries, attn_out, out_grad, row_lse, saved_keys, saved_values
    )
    keyvals = exchanged(keyvals, "y")
    main = lax.all_gather(main, "z", axis=0, tiled=False)
    last = exchanged(last, "z")
    before = attention_backward(main, keyvals)
    me = jnp.bitwise_and(lax.axis_index("z"), 1).reshape(1)
    dq_send, dq_keep, dkv = attention_backward(main, keyvals, last, before, me)

    dkv = exchanged(dkv, TEAM)
    halves = added_up(dkv, tp_count)
    halves = exchanged(halves, TP)
    dq_keep, dq_arrived = rows_by_turns(dq_send, dq_keep)
    key_terms = key_products(halves, source, weight_scale)
    key_terms = exchanged(key_terms, "y")
    blocks = joined(key_terms, dq_keep, dq_arrived)
    blocks = exchanged(blocks, "z")
    query_grad, key_grad = split_sums(blocks, queries.shape[0], source.shape[1])
    halves = halves.reshape(2, tp_count // 2, 2, -1, HEAD_DIM)
    key_half, value_half = (halves[:, :, i].reshape(2, src, HEAD_DIM) for i in range(2))
    weights = jnp.concatenate([key_weight, value_weight], axis=1)
    source_grad = lax.dot_general(
        jnp.concatenate([key_half[0], key_half[1], value_half[0], value_half[1]], axis=1),
        weights,
        (((1,), (1,)), ((), ())),
        preferred_element_type=F32,
    )
    return (query_grad, source_grad, key_grad)


def solution(mesh):
    split = Mesh(mesh.devices.reshape(SPLIT), ("z", "y", "g", "h", "c"))
    return jax.shard_map(
        shards,
        mesh=split,
        in_specs=(
            P(SP, TP),
            P(SP, TP),
            P(SP, TP),
            P(SP, TP),
            P(SP, TP),
            P(SP, None),
            P(SP, None),
            P(TP, None),
            P(TP, None),
        ),
        out_specs=(P(SP, TP), P(SP, TP), P(SP, TP)),
        check_vma=False,
    )
```

```python
import math

import jax
import jax.numpy as jnp
from jax import lax
from jax.experimental import pallas as pl
from jax.experimental.pallas import tpu as pltpu
from jax.sharding import Mesh
from jax.sharding import PartitionSpec as P


HEAD_DIM = 128
SP = ("z", "y")
TP = ("g", "h", "c")
TEAM = ("y", "h", "c")
SPLIT = (16, 4, 2, 2, 2)
F32 = jnp.float32
BF16 = jnp.bfloat16
FIRST = 96
STAT_ROWS = 16
FIRST_VMEM_LIMIT = 24 * 2**20
LAST_VMEM_LIMIT = 24 * 2**20
SMALL_VMEM_LIMIT = 8 * 2**20


def in_vmem():
    return pl.BlockSpec(memory_space=pltpu.VMEM)


def pieces(value):
    high = value.astype(BF16)
    rest = value - high.astype(F32)
    middle = rest.astype(BF16)
    low = (rest - middle.astype(F32)).astype(BF16)
    return [high, middle, low]


def pack_rows(queries, attn_out, out_grad, row_lse, saved_keys, saved_values):
    rows, width = queries.shape
    src = saved_keys.shape[0]
    z_count, y_count = (SPLIT[0], SPLIT[1])

    def kernel(head_ref, q_ref, o_ref, do_ref, lse_ref, k_ref, v_ref, main_ref, last_ref, kv_ref):
        second = head_ref[0] > 0
        main_ref[:rows, :] = q_ref[...]
        main_ref[rows : rows + FIRST, :] = do_ref[:FIRST, :]
        product = do_ref[...].astype(F32) * o_ref[...].astype(F32)
        delta = jnp.sum(product.T, axis=0, keepdims=True)
        stats = pieces(lse_ref[...] * math.sqrt(HEAD_DIM)) + pieces(delta)
        line = lax.broadcasted_iota(jnp.int32, (STAT_ROWS, rows), 0)
        block = jnp.zeros((STAT_ROWS, rows), F32)
        for i, s in enumerate(stats):
            block = jnp.where(line == i, s.astype(F32), block)
        main_ref[rows + FIRST :, :] = block.astype(BF16)
        last = do_ref[FIRST:, :]
        for z in range(z_count):
            last_ref[z] = last
        k = jnp.where(second, k_ref[:, HEAD_DIM:], k_ref[:, :HEAD_DIM])
        v = jnp.where(second, v_ref[:, HEAD_DIM:], v_ref[:, :HEAD_DIM])
        for y in range(y_count):
            kv_ref[y, :src, :] = k
            kv_ref[y, src:, :] = v

    return pl.pallas_call(
        kernel,
        in_specs=[pl.BlockSpec(memory_space=pltpu.SMEM)] + [in_vmem()] * 6,
        out_specs=[in_vmem()] * 3,
        out_shape=[
            jax.ShapeDtypeStruct((rows + FIRST + STAT_ROWS, width), BF16),
            jax.ShapeDtypeStruct((z_count, rows - FIRST, width), BF16),
            jax.ShapeDtypeStruct((y_count, 2 * src, HEAD_DIM), BF16),
        ],
        name="pack_rows",
    )(
        lax.axis_index("g").reshape(1),
        queries,
        attn_out,
        out_grad,
        row_lse.reshape(1, rows),
        saved_keys,
        saved_values,
    )


def dot(left, right):
    return jnp.dot(left, right, preferred_element_type=F32)


def attention_backward(main, keyvals, last=None, before=None, me=None):
    z_count, main_rows, dim = main.shape
    y_count, src = (keyvals.shape[0], keyvals.shape[1] // 2)
    rows = main_rows - FIRST - STAT_ROWS
    low, high = (0, FIRST) if last is None else (FIRST, rows)
    each = high - low
    sources, targets = (y_count * src, z_count * each)
    scale = 1.0 / math.sqrt(HEAD_DIM)
    exp_scale = math.log2(math.e) * scale
    src_tile, tgt_tile = (1024, 512)
    team = y_count * SPLIT[3] * SPLIT[4]
    piece = sources // team

    turned_at = 2 * sources + z_count * FIRST
    queries_at = turned_at + sources
    stats_at = queries_at + z_count * (rows - FIRST)
    handed_rows = stats_at + z_count * (rows - FIRST)

    def prepare(main_ref, kv_ref, last_ref, handed, k_wide, v_wide, k_turned, q_turned, do_turned, q_rows, do_rows):
        lane = lax.broadcasted_iota(jnp.int32, (src, dim), 1)
        lse_lanes = jnp.where(lane < 3, -1.0, 0.0).astype(BF16)
        delta_lanes = jnp.where((lane >= 3) & (lane < 6), -1.0, 0.0).astype(BF16)
        for y in range(y_count):
            at = slice(y * src, (y + 1) * src)
            k = kv_ref[y, :src, :]
            k_wide[at, :dim] = k
            k_wide[at, dim:] = lse_lanes
            v_wide[at, :dim] = kv_ref[y, src:, :]
            v_wide[at, dim:] = delta_lanes
            if last_ref is None:
                k_turned[:, at] = k.T
        if last_ref is None:
            for b in range(0, sources, dim):
                handed[turned_at + b : turned_at + b + dim, :] = k_turned[:, b : b + dim]
        else:
            for b in range(0, sources, dim):
                k_turned[:, b : b + dim] = handed[turned_at + b : turned_at + b + dim, :]
            q_rows[:, :dim] = handed[queries_at:stats_at, :]
            q_rows[:, dim:] = handed[stats_at:handed_rows, :]
        blank = jnp.zeros((dim - STAT_ROWS, dim), BF16)
        for z in range(z_count):
            at = slice(z * each, (z + 1) * each)
            if last_ref is not None:
                do_rows[at, :] = last_ref[z]
                continue
            stats = jnp.concatenate([main_ref[z, rows + FIRST :, :], blank], axis=0).T
            q_rows[at, :dim] = main_ref[z, :FIRST, :]
            q_rows[at, dim:] = stats[:FIRST, :]
            do_rows[at, :] = main_ref[z, rows : rows + FIRST, :]
            other = slice(z * (rows - FIRST), (z + 1) * (rows - FIRST))
            handed[queries_at + other.start : queries_at + other.stop, :] = main_ref[z, FIRST:rows, :]
            handed[stats_at + other.start : stats_at + other.stop, :] = stats[FIRST:, :]
        for b in range(0, targets, dim):
            at = slice(b, b + dim)
            q_turned[:dim, at] = q_rows[at, :dim].T
            stats = q_rows[at, dim:].T
            q_turned[dim:, at] = stats
            do_turned[:dim, at] = do_rows[at, :].T
            do_turned[dim:, at] = stats

    def work(k_wide, v_wide, k_turned, q_turned, do_turned, q_rows, do_rows, dk_acc, dv_acc, dq_acc):
        def step(i, carry):
            s = pl.ds(pl.multiple_of(i * src_tile, src_tile), src_tile)
            for t0 in range(0, targets, tgt_tile):
                t = slice(t0, t0 + tgt_tile)
                scores = dot(k_wide[s, :], q_turned[:, t])
                dprobs = dot(v_wide[s, :], do_turned[:, t])
                probs = jnp.exp2(scores * exp_scale)
                dscores = (probs * dprobs).astype(BF16)
                dv_acc[s, :] += dot(probs.astype(BF16), do_rows[t, :])
                dk_acc[s, :] += dot(dscores, q_rows[t, :dim])
                dq_acc[:, t] += dot(k_turned[:, s], dscores)
            return carry

        dk_acc[...] = jnp.zeros_like(dk_acc)
        dv_acc[...] = jnp.zeros_like(dv_acc)
        dq_acc[...] = jnp.zeros_like(dq_acc)
        lax.fori_loop(0, sources // src_tile, step, 0)

    def first_kernel(main_ref, kv_ref, out_ref, *scratch):
        dk_acc, dv_acc, dq_acc = scratch[-3:]
        prepare(main_ref, kv_ref, None, out_ref, *scratch[:-3])
        work(*scratch)
        out_ref[:sources, :] = (dk_acc[...] * scale).astype(BF16)
        out_ref[sources : 2 * sources, :] = dv_acc[...].astype(BF16)
        for b in range(0, targets, dim):
            turned = (dq_acc[:, b : b + dim] * scale).T.astype(BF16)
            out_ref[2 * sources + b : 2 * sources + b + dim, :] = turned

    def last_kernel(
        me_ref, kv_ref, last_ref, before_ref, send_ref, keep_ref, dkv_ref, *scratch
    ):
        dk_acc, dv_acc, dq_acc, dq_rows = scratch[-4:]
        prepare(None, kv_ref, last_ref, before_ref, *scratch[:-4])
        work(*scratch[:-1])
        for i in range(team):
            at = slice(i * piece, (i + 1) * piece)
            dk_before = before_ref[at, :].astype(F32)
            dv_before = before_ref[sources + i * piece : sources + (i + 1) * piece, :].astype(F32)
            dkv_ref[i, :piece, :] = (dk_acc[at, :] * scale + dk_before).astype(BF16)
            dkv_ref[i, piece:, :] = (dv_acc[at, :] + dv_before).astype(BF16)
        for z in range(z_count // 4):
            at = slice(z * 4 * each, (z + 1) * 4 * each)
            turned = (dq_acc[:, at] * scale).T.astype(BF16)
            for i in range(4):
                dq_rows[z * 4 + i] = turned[i * each : (i + 1) * each, :]
        half_rows = rows // 2
        for odd, (low_ref, high_ref) in enumerate(((keep_ref, send_ref), (send_ref, keep_ref))):

            @pl.when(me_ref[0] == odd)
            def _(low_ref=low_ref, high_ref=high_ref):
                for z in range(z_count):
                    at = 2 * sources + z * FIRST
                    low_ref[z] = before_ref[at : at + half_rows, :]
                    high_ref[z, : FIRST - half_rows, :] = before_ref[at + half_rows : at + FIRST, :]
                high_ref[:, FIRST - half_rows :, :] = dq_rows[...]

    dkv = pltpu.MemorySpace.HBM((team, 2 * piece, dim), BF16)
    scratch = [
        pltpu.VMEM((sources, 2 * dim), BF16),
        pltpu.VMEM((sources, 2 * dim), BF16),
        pltpu.VMEM((dim, sources), BF16),
        pltpu.VMEM((2 * dim, targets), BF16),
        pltpu.VMEM((2 * dim, targets), BF16),
        pltpu.VMEM((targets, 2 * dim), BF16),
        pltpu.VMEM((targets, dim), BF16),
        pltpu.VMEM((sources, dim), F32),
        pltpu.VMEM((sources, dim), F32),
        pltpu.VMEM((dim, targets), F32),
    ]
    if last is None:
        return pl.pallas_call(
            first_kernel,
            in_specs=[in_vmem()] * 2,
            out_specs=in_vmem(),
            out_shape=jax.ShapeDtypeStruct((handed_rows, dim), BF16),
            scratch_shapes=scratch,
            compiler_params=pltpu.CompilerParams(vmem_limit_bytes=FIRST_VMEM_LIMIT),
            name="attention_first",
        )(main, keyvals)
    half = pltpu.MemorySpace.HBM((z_count, rows // 2, dim), BF16)
    return pl.pallas_call(
        last_kernel,
        in_specs=[pl.BlockSpec(memory_space=pltpu.SMEM)] + [in_vmem()] * 3,
        out_specs=[in_vmem()] * 3,
        out_shape=[half, half, dkv],
        scratch_shapes=scratch + [pltpu.VMEM((z_count, each, dim), BF16)],
        compiler_params=pltpu.CompilerParams(vmem_limit_bytes=LAST_VMEM_LIMIT),
        name="attention_last",
    )(me, keyvals, last, before)


def added_up(arrived, copies):
    count, rows, width = arrived.shape

    def kernel(arrived_ref, out_ref):
        total = sum(arrived_ref[i].astype(F32) for i in range(count)).astype(BF16)
        for i in range(copies):
            out_ref[i] = total

    return pl.pallas_call(
        kernel,
        in_specs=[in_vmem()],
        out_specs=in_vmem(),
        out_shape=pltpu.MemorySpace.HBM((copies, rows, width), BF16),
        compiler_params=pltpu.CompilerParams(vmem_limit_bytes=SMALL_VMEM_LIMIT),
        name="added_up",
    )(arrived)


def exchanged(value, axes):
    return lax.all_to_all(value, axes, 0, 0, tiled=True)


def swapped(value, axis, distance):
    pairs = [(i, i ^ distance) for i in range(lax.axis_size(axis))]
    return lax.ppermute(value, axis, pairs)


def rows_by_turns(send, keep):
    arrived = swapped(send, "z", 1)
    for distance in (1, 2):
        count = keep.shape[1] // 2
        mine = jnp.bitwise_and(lax.axis_index("z"), 2 * distance)

        def part(first):
            a, b = (jnp.where(first, v[:, :count], v[:, count:]) for v in (keep, arrived))
            return (a.astype(F32) + b.astype(F32)).astype(BF16)

        send = part(mine > 0)
        keep, arrived = lax.optimization_barrier((keep, arrived))
        keep = part(mine == 0)
        arrived = swapped(send, "z", 2 * distance)
    return keep, arrived


def shuffled(value, outer, middle, inner):
    rows = outer * middle * inner
    new = lax.broadcasted_iota(jnp.int32, (rows, rows), 0)
    old = lax.broadcasted_iota(jnp.int32, (rows, rows), 1)
    m, o, i = (new // (outer * inner), new // inner % outer, new % inner)
    take = old == (o * middle + m) * inner + i
    return dot(jnp.where(take, 1.0, 0.0).astype(BF16), value).astype(BF16)


def key_products(halves, source, weight_scale):
    parts, rows, dim = halves.shape
    z_count, y_count = (SPLIT[0], SPLIT[1])
    own = 2 * dim // (z_count * y_count)

    def kernel(halves_ref, source_ref, out_ref):
        terms = []
        for g in range(2):
            key = jnp.concatenate(
                [halves_ref[g * parts // 2 + p, : rows // 2, :] for p in range(parts // 2)], axis=0
            )
            terms.append(dot(key.T, source_ref[...]))
        terms = (jnp.concatenate(terms, axis=0) * weight_scale).astype(BF16)
        terms = shuffled(terms, z_count, y_count, own)
        for y in range(y_count):
            out_ref[y] = terms[y * z_count * own : (y + 1) * z_count * own, :]

    return pl.pallas_call(
        kernel,
        in_specs=[in_vmem()] * 2,
        out_specs=in_vmem(),
        out_shape=jax.ShapeDtypeStruct((y_count, z_count * own, source.shape[1]), BF16),
        compiler_params=pltpu.CompilerParams(vmem_limit_bytes=SMALL_VMEM_LIMIT),
        name="key_products",
    )(halves, source)


def joined(keys, keep, arrived):
    y_count, rows, width = keys.shape
    z_count, share, dim = keep.shape
    own = rows // z_count
    wide = width // dim

    def kernel(keys_ref, keep_ref, arrived_ref, out_ref):
        total = sum(keys_ref[y].astype(F32) for y in range(y_count)).astype(BF16)
        blocks = [total[:, b * dim : (b + 1) * dim] for b in range(wide)]
        blocks = shuffled(jnp.concatenate(blocks, axis=0), wide, z_count, own)
        dq = keep_ref[...].astype(F32) + arrived_ref[...].astype(F32)
        out_ref[:, :share, :] = dq.astype(BF16)
        for z in range(z_count):
            out_ref[z, share:, :] = blocks[z * wide * own : (z + 1) * wide * own, :]

    return pl.pallas_call(
        kernel,
        in_specs=[in_vmem()] * 3,
        out_specs=in_vmem(),
        out_shape=jax.ShapeDtypeStruct((z_count, share + wide * own, dim), BF16),
        compiler_params=pltpu.CompilerParams(vmem_limit_bytes=SMALL_VMEM_LIMIT),
        name="joined",
    )(keys, keep, arrived)


def split_sums(blocks, rows, width):
    z_count, height, dim = blocks.shape
    share = rows // 8
    wide = width // dim
    own = (height - share) // wide

    def kernel(blocks_ref, dq_ref, keys_ref):
        for turn in range(8):
            first = turn % 2 * 4 + turn // 2 % 2 * 2 + turn // 4
            dq_ref[first * share : (first + 1) * share, :] = sum(
                blocks_ref[z, :share, :].astype(F32) for z in range(turn, z_count, 8)
            )
        keys = sum(blocks_ref[z, share:, :].astype(F32) for z in range(z_count))
        for b in range(wide):
            keys_ref[:, b * dim : (b + 1) * dim] = keys[b * own : (b + 1) * own, :]

    return pl.pallas_call(
        kernel,
        in_specs=[in_vmem()],
        out_specs=[in_vmem()] * 2,
        out_shape=[
            jax.ShapeDtypeStruct((rows, dim), F32),
            jax.ShapeDtypeStruct((own, width), F32),
        ],
        compiler_params=pltpu.CompilerParams(vmem_limit_bytes=SMALL_VMEM_LIMIT),
        name="split_sums",
    )(blocks)


def shards(
    queries, attn_out, out_grad, row_lse, source, saved_keys, saved_values, key_weight, value_weight
):
    src = source.shape[0]
    tp_count = SPLIT[2] * SPLIT[3] * SPLIT[4]
    sp_count = SPLIT[0] * SPLIT[1]
    weight_scale = 1.0 / math.sqrt(src * sp_count)
    main, last, keyvals = pack_rows(
        queries, attn_out, out_grad, row_lse, saved_keys, saved_values
    )
    keyvals = exchanged(keyvals, "y")
    main = lax.all_gather(main, "z", axis=0, tiled=False)
    last = exchanged(last, "z")
    before = attention_backward(main, keyvals)
    me = jnp.bitwise_and(lax.axis_index("z"), 1).reshape(1)
    dq_send, dq_keep, dkv = attention_backward(main, keyvals, last, before, me)

    dkv = exchanged(dkv, TEAM)
    halves = added_up(dkv, tp_count)
    halves = exchanged(halves, TP)
    dq_keep, dq_arrived = rows_by_turns(dq_send, dq_keep)
    key_terms = key_products(halves, source, weight_scale)
    key_terms = exchanged(key_terms, "y")
    blocks = joined(key_terms, dq_keep, dq_arrived)
    blocks = exchanged(blocks, "z")
    query_grad, key_grad = split_sums(blocks, queries.shape[0], source.shape[1])
    halves = halves.reshape(2, tp_count // 2, 2, -1, HEAD_DIM)
    key_half, value_half = (halves[:, :, i].reshape(2, src, HEAD_DIM) for i in range(2))
    weights = jnp.concatenate([key_weight, value_weight], axis=1)
    source_grad = lax.dot_general(
        jnp.concatenate([key_half[0], key_half[1], value_half[0], value_half[1]], axis=1),
        weights,
        (((1,), (1,)), ((), ())),
        preferred_element_type=F32,
    )
    return (query_grad, source_grad, key_grad)


def solution(mesh):
    split = Mesh(mesh.devices.reshape(SPLIT), ("z", "y", "g", "h", "c"))
    return jax.shard_map(
        shards,
        mesh=split,
        in_specs=(
            P(SP, TP),
            P(SP, TP),
            P(SP, TP),
            P(SP, TP),
            P(SP, TP),
            P(SP, None),
            P(SP, None),
            P(TP, None),
            P(TP, None),
        ),
        out_specs=(P(SP, TP), P(SP, TP), P(SP, TP)),
        check_vma=False,
    )
```
